512 devices in a mesh: sp: 32 (over z, x), tp: 16 (over y, core).
Axes of the slice: x: 4, y: 8, z: 8, core: 2. Of those that a mesh axis runs over, the one named last changes fastest.
Arguments:
- residual_in: bfloat16 [4096, 2048], P('sp', 'tp'), may hold values from -8 to 8
- query_alpha: bfloat16 [4096, 2048], P('sp', 'tp'), may hold values from -8 to 8
- pairs_alpha: bfloat16 [4096, 16, 128], P('sp', 'tp'), may hold values from -8 to 8
- offset_alpha: float32 [4096, 32], P('sp', 'tp'), may hold values from -18 to -1
- gain_alpha: float32 [2048], P('tp'), may hold values from 0.1 to 1.9
- query_beta: bfloat16 [4096, 2048], P('sp', 'tp'), may hold values from -8 to 8
- pairs_beta: bfloat16 [4096, 16, 256], P('sp', 'tp'), may hold values from -8 to 8
- offset_beta: float32 [4096, 16], P('sp', 'tp'), may hold values from -18 to -1
- gain_beta: float32 [2048], P('tp'), may hold values from 0.1 to 1.9
- project_alpha: bfloat16 [2048, 2048], P('tp'), may hold values from -0.09375 to 0.09375
- project_beta: bfloat16 [2048, 2048], P('tp'), may hold values from -0.09375 to 0.09375
- gain_settle: float32 [2048], P('tp'), may hold values from 0 to 4
- bias_settle: float32 [2048], P('tp'), may hold values from -2.5 to 2.5
- expert_ids: int32 [4096, 2], P('sp'), may hold values from 0 to 31, as said below
- route_weight: float32 [4096, 2], P('sp'), may hold values from 0.1 to 0.9
- expert_gate: bfloat16 [32, 2048, 4096], P('sp', None, 'tp'), may hold values from -0.125 to 0.125
- expert_up: bfloat16 [32, 2048, 4096], P('sp', None, 'tp'), may hold values from -0.125 to 0.125
- expert_down: bfloat16 [32, 4096, 2048], P('sp', 'tp'), may hold values from -0.1875 to 0.1875
- gain_final: float32 [2048], P('tp'), may hold values from 0.1 to 1.9
- bias_final: float32 [2048], P('tp'), may hold values from -2.5 to 2.5
Outputs:
- layer_out: bfloat16 [4096, 2048], P('sp', 'tp')
The draws below stay inside these ranges and needn't reach their ends.
Inputs may be any that keep to these rules, and one draw needn't show every extreme that they name: `expert_ids`: the two numbers of a row differ and lie in one group of 8 consecutive experts. Among the rows of one device, no expert is named more than 12 times, and every expert of one group, the same group for all devices, is named exactly 12 times.
All inputs are finite; a program needn't handle non-finite values.
Results may differ from the reference program's by a relative error of at most 0.018.
Values may be sent and summed in bfloat16 or wider, within the bound.
A program may use at most 64 MiB of HBM per device.

```python
import math
import jax
import jax.numpy as jnp
from jax import lax

D = 2048
HA = 32
DA = 64
HKA = 16
HB = 16
DB = 128
FFE = 4096
GROUPS = 4
TOK_DEV = 128
TOKEN_COUNT = 4096
EXPERTS = 32
EPG = 8
CAP = 12
HEAVY = 48
N_SP = 32
N_TP = 16


def rising(count, top):
    return top ** (jnp.arange(count, dtype=jnp.float32) / (count - 1))


def draw_residual_in(key, part):
    stream = jax.random.fold_in(key, 11)
    anchor_figure = jnp.clip(jax.random.normal(stream, (TOKEN_COUNT, D), jnp.float32), -4.0, 4.0)
    scale = rising(D, 3.0) / 1.7
    return (anchor_figure * scale[None, :]).astype(jnp.bfloat16)


def pair_draw(key, heads, width):
    first, second = jax.random.split(key)
    keys = 1.6 * jnp.clip(jax.random.normal(first, (TOKEN_COUNT, heads, width), jnp.float32), -4.0, 4.0)
    values = jnp.clip(jax.random.normal(second, (TOKEN_COUNT, heads, width), jnp.float32), -4.0, 4.0)
    values = values * (rising(heads, 3.0) / 1.7)[None, :, None]
    return jnp.concatenate([keys, values], axis=2).astype(jnp.bfloat16)


def draw_pairs_alpha(key, part):
    return pair_draw(jax.random.fold_in(key, 21), HKA, DA)


def draw_pairs_beta(key, part):
    return pair_draw(jax.random.fold_in(key, 22), HB, DB)


def offset_draw(key, heads):
    streams = jax.random.split(key, 7)
    blocks = TOKEN_COUNT // TOK_DEV
    share = 0.5
    fast = jax.random.uniform(streams[0], (heads,), jnp.float32) < share
    slow_base = -math.log(TOKEN_COUNT) - 3.3 - jax.random.uniform(streams[1], (heads,), jnp.float32, 0.5, 2.5)
    fast_base = -math.log(40.0) - 3.3 + jax.random.uniform(streams[2], (heads,), jnp.float32, -0.5, 0.5)
    anchor_figure = jnp.where(fast, fast_base, slow_base)
    slope_figure = jnp.repeat(jax.random.uniform(streams[3], (blocks, heads), jnp.float32, -0.7, 0.7), TOK_DEV, axis=0)
    coarse_estimate = jax.random.uniform(streams[4], (TOKEN_COUNT, heads), jnp.float32, -0.4, 0.4)
    marked_places = jax.random.randint(streams[5], (3, heads), 1, TOKEN_COUNT)
    sudden_jump_figure = jnp.any(jnp.arange(TOKEN_COUNT)[:, None, None] == marked_places[None, :, :], axis=1)
    dominant_figure = jax.random.uniform(streams[6], (TOKEN_COUNT, heads), jnp.float32, -2.5, -1.0)
    return jnp.where(sudden_jump_figure, dominant_figure, anchor_figure[None, :] + slope_figure + coarse_estimate).astype(jnp.float32)


def draw_offset_alpha(key, part):
    return offset_draw(jax.random.fold_in(key, 31), HA)


def draw_offset_beta(key, part):
    return offset_draw(jax.random.fold_in(key, 32), HB)


def draw_gain_settle(key, part):
    stream = jax.random.fold_in(key, 41)
    anchor_figure = 1.0 + 0.18 * jax.random.uniform(stream, (D,), jnp.float32, -1.0, 1.0)
    scale = rising(D, 3.0) / 1.7
    return (anchor_figure * scale).astype(jnp.float32)


def draw_expert_ids(key, part):
    blocks = TOKEN_COUNT // TOK_DEV
    heavy_group = jax.random.randint(jax.random.fold_in(key, 51), (), 0, GROUPS)

    def one_block(block_key):
        streams = jax.random.split(block_key, 5)
        rank = jax.random.permutation(streams[0], TOK_DEV)
        offset = jax.random.randint(streams[1], (GROUPS,), 0, EPG)
        stride = jax.random.randint(streams[2], (GROUPS,), 1, EPG)
        rotate = jax.random.randint(streams[3], (), 0, GROUPS - 1)
        flip = jax.random.randint(streams[4], (TOK_DEV,), 0, 2)
        in_heavy = rank < HEAVY
        rest = rank - HEAVY
        other = (heavy_group + 1 + (rest % (GROUPS - 1) + rotate) % (GROUPS - 1)) % GROUPS
        group = jnp.where(in_heavy, heavy_group, other)
        index = jnp.where(in_heavy, rank, rest // (GROUPS - 1))
        lead = group * EPG + (offset[group] + index) % EPG
        trail = group * EPG + (offset[group] + index + stride[group]) % EPG
        left = jnp.where(flip == 1, trail, lead)
        right = jnp.where(flip == 1, lead, trail)
        return jnp.stack([left, right], axis=1)
    ids = jax.vmap(one_block)(jax.random.split(jax.random.fold_in(key, 52), blocks))
    return ids.reshape(TOKEN_COUNT, 2).astype(jnp.int32)


def shard_levels(own_key, shape, shards, low, largest):
    def one(position, blocks):
        heights = jax.random.uniform(jax.random.fold_in(jax.random.fold_in(own_key, 6), position), (blocks,), jnp.float32, low / len(shards), largest / len(shards))
        return jnp.repeat(jnp.exp(heights), shape[position] // blocks).reshape((-1,) + (1,) * (len(shape) - position - 1))

    level = one(*shards[0])
    for cut in shards[1:]:
        level = level * one(*cut)
    return level


def noise(own_key, extent, deviation, most, cuts=(), kind=jnp.bfloat16):
    drawn = deviation * jax.random.normal(own_key, extent, jnp.float32)
    if cuts:
        drawn = drawn * shard_levels(own_key, extent, cuts, -0.22, 0.18)
    return jnp.clip(drawn, -most, most).astype(kind)


def setup_inputs(seed: int = 0) -> dict:
    arg_keys = jax.random.split(jax.random.key(seed), 21)
    residual_in = draw_residual_in(jax.random.fold_in(arg_keys[20], 71), 0)
    query_alpha = noise(arg_keys[1], (TOKEN_COUNT, HA * DA), 1.6, 8.0, ((0, 32), (1, 16)))
    pairs_alpha = draw_pairs_alpha(jax.random.fold_in(arg_keys[20], 71), 0)
    offset_alpha = draw_offset_alpha(jax.random.fold_in(arg_keys[20], 71), 0)
    gain_alpha = jnp.clip(1.0 + 0.18 * jax.random.normal(arg_keys[4], (HA * DA,), jnp.float32), 0.1, 1.9)
    query_beta = noise(arg_keys[5], (TOKEN_COUNT, HB * DB), 1.6, 8.0, ((0, 32), (1, 16)))
    pairs_beta = draw_pairs_beta(jax.random.fold_in(arg_keys[20], 71), 0)
    offset_beta = draw_offset_beta(jax.random.fold_in(arg_keys[20], 71), 0)
    gain_beta = jnp.clip(1.0 + 0.18 * jax.random.normal(arg_keys[8], (HB * DB,), jnp.float32), 0.1, 1.9)
    project_alpha = noise(arg_keys[9], (HA * DA, D), (HA * DA + HB * DB) ** -0.5, 0.09375, ((0, 16),))
    project_beta = noise(arg_keys[10], (HB * DB, D), (HA * DA + HB * DB) ** -0.5, 0.09375, ((0, 16),))
    gain_settle = draw_gain_settle(jax.random.fold_in(arg_keys[20], 71), 0)
    bias_settle = noise(arg_keys[12], (D,), 0.5, 2.5, ((0, 16),), jnp.float32)
    expert_ids = draw_expert_ids(jax.random.fold_in(arg_keys[20], 71), 0)
    route_weight = jnp.clip(0.1 + 0.79999997 * jax.random.uniform(arg_keys[14], (TOKEN_COUNT, 2), jnp.float32) ** shard_levels(arg_keys[14], (TOKEN_COUNT, 2), ((0, 32),), -0.2, 0.2), 0.1, 0.9)
    expert_gate = noise(arg_keys[15], (EXPERTS, D, FFE), D ** -0.5, 0.125, ((0, 32), (2, 16)))
    expert_up = noise(arg_keys[16], (EXPERTS, D, FFE), D ** -0.5, 0.125, ((0, 32), (2, 16)))
    expert_down = noise(arg_keys[17], (EXPERTS, FFE, D), (FFE // 4) ** -0.5, 0.1875, ((0, 32), (1, 16)))
    gain_final = jnp.clip(1.0 + 0.18 * jax.random.normal(arg_keys[18], (D,), jnp.float32), 0.1, 1.9)
    bias_final = noise(arg_keys[19], (D,), 0.5, 2.5, ((0, 16),), jnp.float32)
    return dict(residual_in=residual_in, query_alpha=query_alpha, pairs_alpha=pairs_alpha, offset_alpha=offset_alpha, gain_alpha=gain_alpha, query_beta=query_beta, pairs_beta=pairs_beta, offset_beta=offset_beta, gain_beta=gain_beta, project_alpha=project_alpha, project_beta=project_beta, gain_settle=gain_settle, bias_settle=bias_settle, expert_ids=expert_ids, route_weight=route_weight, expert_gate=expert_gate, expert_up=expert_up, expert_down=expert_down, gain_final=gain_final, bias_final=bias_final)


depth_scale = 2.0 ** 0.5
norm_eps = 1e-05

def stick_heads(queries, pairs, offsets, heads, kv_heads, width):
    share = heads // kv_heads
    q_heads = jnp.transpose(queries.reshape(TOKEN_COUNT, heads, width), (1, 0, 2))
    k_heads = jnp.transpose(pairs[:, :, :width], (1, 0, 2))
    v_heads = jnp.transpose(pairs[:, :, width:], (1, 0, 2))
    scale = width ** (-0.5)
    key_pos = jnp.arange(TOKEN_COUNT, dtype=jnp.int32)
    firsts = jnp.arange(TOKEN_COUNT // TOK_DEV, dtype=jnp.int32) * TOK_DEV

    def one_head(args):
        q_all, bias, index = args
        keys = k_heads[index // share]
        values = v_heads[index // share]
        blocks = q_all.reshape(TOKEN_COUNT // TOK_DEV, TOK_DEV, width)

        def one_block(inner):
            q_rows, first = inner
            scores = jnp.dot(q_rows, keys.T, preferred_element_type=jnp.float32) * scale + bias[None, :]
            query_pos = first + jnp.arange(TOK_DEV, dtype=jnp.int32)
            valid = key_pos[None, :] < query_pos[:, None]
            soft = jnp.where(valid, jax.nn.softplus(scores), 0.0)
            later = lax.cumsum(soft, axis=1, reverse=True) - soft
            weights = jnp.where(valid, jnp.exp(jax.nn.log_sigmoid(scores) - later), 0.0).astype(jnp.bfloat16)
            return jnp.dot(weights, values, preferred_element_type=jnp.float32)
        return lax.map(one_block, (blocks, firsts)).reshape(TOKEN_COUNT, width)
    out = lax.map(one_head, (q_heads, jnp.transpose(offsets), jnp.arange(heads, dtype=jnp.int32)))
    return jnp.transpose(out, (1, 0, 2)).reshape(TOKEN_COUNT, heads * width)

def group_norm(attend, gain):
    mean_sq = lax.optimization_barrier(jnp.mean(attend * attend, axis=1, keepdims=True))
    return (attend * lax.rsqrt(mean_sq + norm_eps) * gain).astype(jnp.bfloat16)

def shard_sum(products, count):

    def add_piece(total, index):
        term = jnp.zeros((count, D), jnp.float32)
        for left, right in products:
            width = left.shape[1] // N_TP
            piece = lax.dynamic_slice_in_dim(left, index * width, width, 1)
            block = lax.dynamic_slice_in_dim(right, index * width, width, 0)
            term = term + jnp.dot(piece, block, preferred_element_type=jnp.float32)
        rounded = lax.optimization_barrier(term.astype(jnp.bfloat16))
        return (total + rounded.astype(jnp.float32), None)
    total, _ = lax.scan(add_piece, jnp.zeros((count, D), jnp.float32), jnp.arange(N_TP, dtype=jnp.int32))
    return total

def layer_norm(total, gain, bias):
    mean = lax.optimization_barrier(jnp.sum(total, axis=1, keepdims=True)) / D
    var = lax.optimization_barrier(jnp.sum(total * total, axis=1, keepdims=True)) / D - mean * mean
    return ((total - mean) * lax.rsqrt(var + norm_eps) * gain + bias).astype(jnp.bfloat16)

def reference(residual_in, query_alpha, pairs_alpha, offset_alpha, gain_alpha, query_beta, pairs_beta, offset_beta, gain_beta, project_alpha, project_beta, gain_settle, bias_settle, expert_ids, route_weight, expert_gate, expert_up, expert_down, gain_final, bias_final):
    attend_alpha = stick_heads(query_alpha, pairs_alpha, offset_alpha, HA, HKA, DA)
    attend_beta = stick_heads(query_beta, pairs_beta, offset_beta, HB, HB, DB)
    normed_alpha = group_norm(attend_alpha, gain_alpha)
    normed_beta = group_norm(attend_beta, gain_beta)
    mixed = shard_sum(((normed_alpha, project_alpha), (normed_beta, project_beta)), TOKEN_COUNT).astype(jnp.bfloat16)
    first = depth_scale * residual_in.astype(jnp.float32) + mixed.astype(jnp.float32)
    settled = layer_norm(first, gain_settle, bias_settle)
    ids = expert_ids.reshape(N_SP, 2 * TOK_DEV)
    onehot = (ids[:, :, None] == jnp.arange(EXPERTS, dtype=jnp.int32)[None, None, :]).astype(jnp.int32)
    before = jnp.cumsum(onehot, axis=1, dtype=jnp.int32) - onehot
    slot = lax.optimization_barrier(jnp.sum(before * onehot, axis=2, dtype=jnp.int32))
    place = (jnp.arange(N_SP, dtype=jnp.int32)[:, None] * CAP + slot).reshape(TOKEN_COUNT * 2)
    owner = jnp.arange(TOKEN_COUNT * 2, dtype=jnp.int32) // 2
    table = jnp.full((EXPERTS, N_SP * CAP), TOKEN_COUNT, jnp.int32).at[expert_ids.reshape(TOKEN_COUNT * 2), place].set(owner)
    padded = jnp.concatenate([settled, jnp.zeros((1, D), jnp.bfloat16)], axis=0)

    def one_expert(args):
        rows, gate_w, up_w, down_w = args
        inputs = padded[rows]
        gate = jnp.dot(inputs, gate_w, preferred_element_type=jnp.float32)
        up = jnp.dot(inputs, up_w, preferred_element_type=jnp.float32)
        hidden = (jax.nn.silu(gate) * up).astype(jnp.bfloat16)
        return shard_sum(((hidden, down_w),), N_SP * CAP).astype(jnp.bfloat16)
    outputs = lax.map(one_expert, (table, expert_gate, expert_up, expert_down))
    picked = outputs[expert_ids, place.reshape(TOKEN_COUNT, 2)].astype(jnp.float32)
    routed = route_weight[:, 0:1] * picked[:, 0] + route_weight[:, 1:2] * picked[:, 1]
    second = depth_scale * settled.astype(jnp.float32) + routed
    return layer_norm(second, gain_final, bias_final)
```

```python
import functools
import jax
import jax.numpy as jnp
from jax import lax
from jax.experimental import pallas as pl
from jax.experimental.pallas import tpu as pltpu
from jax.sharding import PartitionSpec as P

depth_scale = 2.0**0.5
norm_eps = 1e-05
MESH = pl.DeviceIdType.MESH
NX = 4
CAP = 12
STRIDE = 16
bf16 = jnp.bfloat16
f32 = jnp.float32


def iota(shape, dim):
    return lax.broadcasted_iota(jnp.int32, shape, dim)


def ones_where(cond):
    return jnp.where(cond, 1.0, 0.0).astype(bf16)


def dot(a, b):
    return jnp.dot(a, b, preferred_element_type=f32)


def dot_tr(a, b):
    return lax.dot_general(a, b, (((1,), (1,)), ((), ())), preferred_element_type=f32)


def dot_tl(a, b):
    return lax.dot_general(a, b, (((0,), (0,)), ((), ())), preferred_element_type=f32)


def split(v, pieces):
    found = []
    for _ in range(pieces):
        part = v.astype(bf16)
        found.append(part)
        v = v - part.astype(f32)
    return found


def spread(rows8, low, high):
    parts = [p.astype(f32) for p in split(rows8, 3)] + [jnp.zeros_like(rows8)]
    stacked = jnp.concatenate(parts, axis=0).astype(bf16)
    row = iota((32, 256), 0)
    lane = iota((32, 256), 1)
    slot = row & 7
    pick = jnp.zeros((32, 256), jnp.bool_)
    for r, (first, last) in zip(low, high):
        pick = pick | ((slot == r) & (lane >= first) & (lane < last) & (row < 24))
    return dot_tl(stacked, ones_where(pick))


def rowsums(v):
    cat = jnp.concatenate(split(v, 3), axis=1)
    lane = iota((8, 768), 1) & 255
    row = iota((8, 768), 0)
    return dot_tr(ones_where((lane < 128) == (row < 4)), cat)


def rcopy(src, dst, send, recv, sp, tp):
    return pltpu.make_async_remote_copy(
        src_ref=src, dst_ref=dst, send_sem=send, recv_sem=recv, device_id=(sp, tp), device_id_type=MESH
    )


def loop(low, high, step):
    def run(i, carry):
        step(i)
        return carry

    lax.fori_loop(low, high, run, 0)


def attend_kernel(
    nz, qa_ref, qb_ref, ka_ref, kb_ref, off_ref, out_ref,
    kva, kvr, kvb, off, qba, qbb, ret, back, tot, tback,
    ks, kr, qs, qr, rs, rr,
):
    sp, tp = lax.axis_index("sp"), lax.axis_index("tp")
    z, x = lax.div(sp, NX), lax.rem(sp, NX)

    barrier = pltpu.get_barrier_semaphore()

    def greet_x(d):
        pl.semaphore_signal(barrier, 1, device_id=(z * NX + lax.rem(x + d, NX), tp), device_id_type=MESH)

    def greet_z(d):
        pl.semaphore_signal(barrier, 1, device_id=(lax.rem(z + d, nz) * NX + x, tp), device_id_type=MESH)

    loop(1, NX, greet_x)
    loop(1, nz, greet_z)
    pl.semaphore_wait(barrier, NX - 1 + nz - 1)

    def key_copies(d, src_x):
        peer = z * NX + lax.rem(x + d, NX)
        rows = pl.ds(pl.multiple_of(src_x * 128, 128), 128)
        return (
            rcopy(ka_ref, kva.at[rows, :], ks.at[0, d], kr.at[0, d], peer, tp),
            rcopy(kb_ref, kvb.at[rows, :], ks.at[1, d], kr.at[1, d], peer, tp),
            rcopy(off_ref, off.at[:, rows], ks.at[2, d], kr.at[2, d], peer, tp),
        )

    def query_copies(dst_z, src_z):
        peer = dst_z * NX + x
        return (
            rcopy(qa_ref, qba.at[src_z], qs.at[0, dst_z], qr.at[0, src_z], peer, tp),
            rcopy(qb_ref, qbb.at[src_z], qs.at[1, dst_z], qr.at[1, src_z], peer, tp),
        )

    def result_copies(dst_z, src_z):
        peer = dst_z * NX + x
        return (
            rcopy(ret.at[dst_z], back.at[src_z], rs.at[0, dst_z], rr.at[0, src_z], peer, tp),
            rcopy(tot.at[dst_z], tback.at[src_z], rs.at[1, dst_z], rr.at[1, src_z], peer, tp),
        )

    def send_keys(d):
        for c in key_copies(d, x):
            c.start()

    loop(1, NX, send_keys)

    def send_query(k):
        for c in query_copies(z - 1 - k, z):
            c.start()

    loop(0, z, send_query)

    mine = pl.ds(pl.multiple_of(x * 128, 128), 128)
    kva[mine, :] = ka_ref[...]
    kvb[mine, :] = kb_ref[...]
    off[:, mine] = off_ref[...]
    qba[z] = qa_ref[...]
    qbb[z] = qb_ref[...]

    def await_keys(d):
        for c in key_copies(d, lax.rem(x - d + NX, NX)):
            c.wait_recv()

    loop(1, NX, await_keys)
    keys_a = kva[...]
    kvr[...] = pltpu.roll(keys_a.astype(f32), 64, 1).astype(bf16)

    lane = iota((128, 128), 1)
    gap = lane - iota((128, 128), 0)
    r256, c256 = iota((256, 256), 0) & 127, iota((256, 256), 1)
    later_matrix = ones_where((r256 > c256) | (c256 >= 128))
    ones8 = jnp.ones((8, 256), bf16)
    row8 = iota((8, 128), 0)

    def visit(zq):
        @pl.when(zq > z)
        def _():
            for c in query_copies(z, zq):
                c.wait_recv()

        qa, qb = qba[zq], qbb[zq]
        zero = jnp.zeros_like(qa)
        accs, totals = [], []
        for h in range(3):
            q = (jnp.where(lane < 64, qa, zero), jnp.where(lane >= 64, qa, zero), qb)[h]
            scale = (64.0**-0.5, 64.0**-0.5, 128.0**-0.5)[h]
            gone = jnp.zeros((128, 128), f32)
            total = jnp.zeros((8, 128), f32)
            weights = [None] * NX
            for b in reversed(range(NX)):
                rows = slice(b * 128, b * 128 + 128)
                keys = (kva[rows, :], kvr[rows, :], kvb[rows, :128])[h]
                scores = dot_tr(q, keys) * scale + off[h : h + 1, rows]
                valid = gap < (zq - z) * (NX * 128) + (x - b) * 128
                soft = jnp.maximum(scores, 0.0) + jnp.log(1.0 + jnp.exp(-jnp.abs(scores)))
                cat = jnp.concatenate(split(jnp.where(valid, soft, 0.0), 2), axis=1)
                sums = dot(cat, later_matrix)
                total = total + dot_tr(ones8, cat)
                power = (scores - soft) - (sums[:, :128] + gone)
                gone = gone + sums[:, 128:]
                weights[b] = jnp.where(valid, jnp.exp(power), 0.0).astype(bf16)
            values = (kvr[...], kva[...], kvb[:, 128:])[h]
            accs.append(dot(jnp.concatenate(weights, axis=1), values))
            totals.append(total)
        both = jnp.where(lane < 64, accs[0], accs[1])
        found = jnp.concatenate([both, accs[2]], axis=1).astype(bf16)
        sums8 = jnp.where(row8 == 0, totals[0], jnp.where(row8 == 1, totals[1], totals[2]))

        @pl.when(zq == z)
        def _():
            back[z] = found
            tback[z] = sums8

        @pl.when(zq > z)
        def _():
            ret[zq] = found
            tot[zq] = sums8
            for c in result_copies(zq, z):
                c.start()

    loop(z, nz, visit)

    def gather(k, carry):
        acc, gone = carry
        zk = z - k

        @pl.when(k > 0)
        def _():
            for c in result_copies(z, zk):
                c.wait_recv()

        wide = spread(jnp.exp(-gone), (0, 1, 2), ((0, 64), (64, 128), (128, 256)))
        return acc + wide * back[zk].astype(f32), gone + tback[zk]

    acc, _ = lax.fori_loop(
        0, z + 1, gather, (jnp.zeros((128, 256), f32), jnp.zeros((8, 128), f32))
    )
    out_ref[...] = acc

    def end_keys(d):
        for c in key_copies(d, x):
            c.wait_send()

    def end_query(k):
        for c in query_copies(z - 1 - k, z):
            c.wait_send()

    def end_result(zq):
        for c in result_copies(zq, z):
            c.wait_send()

    loop(1, NX, end_keys)
    loop(0, z, end_query)
    loop(z + 1, nz, end_result)


def near_order(n):
    return sorted(range(1, n), key=lambda d: (min(d, n - d), d))


def layer_kernel(
    nsp, ntp,
    att_ref, res_ref, ga_ref, gb_ref, gs_ref, bs_ref, gf_ref, bf_ref, ids_ref, route_ref,
    pa_hbm, pb_hbm, wg_hbm, wu_hbm, wd_hbm, out_ref,
    pa, pb, wg, wu, wd, wsem,
    stat, stats, ss, sr,
    p1s, p1o, p1v, p1r, p1i, p1ss, p1sr, p1rs, p1rr,
    dsp, drv, ds_, dr_,
    xg, gs2, gr2, fs2, fr2, acc_g, acc_u,
    p2s, p2o, p2v, p2r, p2i, p2ss, p2sr, p2rs, p2rr,
    rts, rtv, ts_, tr_,
):
    sp, tp = lax.axis_index("sp"), lax.axis_index("tp")
    ny = ntp // 2
    y, c = lax.div(tp, 2), lax.rem(tp, 2)
    mate = y * 2 + 1 - c
    columns = ntp * 128

    loads = [
        pltpu.make_async_copy(src, dst, wsem.at[i])
        for i, (src, dst) in enumerate(
            ((pa_hbm, pa), (pb_hbm, pb), (wg_hbm, wg), (wu_hbm, wu), (wd_hbm, wd))
        )
    ]
    for load in loads:
        load.start()

    barrier = pltpu.get_barrier_semaphore()

    def greet_sp(d):
        pl.semaphore_signal(barrier, 1, device_id=(lax.rem(sp + d, nsp), tp), device_id_type=MESH)

    def greet_tp(d):
        pl.semaphore_signal(barrier, 1, device_id=(sp, lax.rem(tp + d, ntp)), device_id_type=MESH)

    loop(1, nsp, greet_sp)
    loop(1, ntp, greet_tp)
    pl.semaphore_wait(barrier, nsp - 1 + ntp - 1)

    def stat_copy(n, d):
        return rcopy(stat.at[n], stats.at[n, d], ss.at[n, d], sr.at[n, d], sp, lax.rem(tp + d, ntp))

    def over_tp(n, rows8):
        stat[n] = rows8
        loop(1, ntp, lambda d: stat_copy(n, d).start())
        loop(1, ntp, lambda d: stat_copy(n, d).wait_recv())
        total = rows8
        for d in range(1, ntp):
            total = total + stats[n, d]
        return total

    def summed(product, sent, own, from_mate, reduced, arrived, sem_ms, sem_mr, sem_s, sem_r):
        def to_mate(d):
            return rcopy(sent.at[d], from_mate.at[d], sem_ms.at[d], sem_mr.at[d], sp, mate)

        def to_chip(d):
            return rcopy(
                reduced.at[d], arrived.at[d], sem_s.at[d], sem_r.at[d], sp, lax.rem(y + d, ny) * 2 + c
            )

        def make(d):
            both = product(lax.rem(y + d, ny))
            left, right = both[:, :128], both[:, 128:]
            sent[d] = jnp.where(c == 0, right, left).astype(bf16)
            to_mate(d).start()
            own[d] = jnp.where(c == 0, left, right)

        def pass_on(d):
            to_mate(d).wait_recv()
            reduced[d] = (own[d] + from_mate[d].astype(f32)).astype(bf16)
            to_chip(d).start()

        order = near_order(ny)[::-1]
        make(order[0])
        for before, d in zip(order, order[1:] + [0]):
            make(d)
            pass_on(before)
        to_mate(0).wait_recv()
        total = own[0] + from_mate[0].astype(f32)
        for d in order[::-1]:
            to_chip(d).wait_recv()
            total = total + arrived[d].astype(f32)
        return total, to_mate, to_chip

    lane128 = iota((128, 128), 1)
    hot = [ids_ref[:, k : k + 1] == lane128 for k in range(2)]
    tri = ones_where(iota((128, 128), 0) > lane128)
    earlier = dot(tri, ones_where(hot[0] | hot[1]))
    lane_all = iota((128, nsp * STRIDE), 1).astype(f32)
    choice = []
    for k in range(2):
        slot = jnp.sum(jnp.where(hot[k], earlier, 0.0), axis=1, keepdims=True)
        place = ids_ref[:, k : k + 1].astype(f32) * float(STRIDE) + slot
        choice.append(ones_where(place == lane_all))
    row_c, col_c = iota((nsp * CAP, nsp * STRIDE), 0), iota((nsp * CAP, nsp * STRIDE), 1)
    block_c = (row_c * (-(-(1 << 17) // CAP))) >> 17
    compact = ones_where(col_c == row_c + block_c * (STRIDE - CAP))

    attend = att_ref[...]
    squares = over_tp(0, rowsums(attend * attend))
    halves = ((0, 128), (128, 256))
    scale = spread(lax.rsqrt(squares / float(columns) + norm_eps), (0, 4), halves)
    normed_a = (attend[:, :128] * scale[:, :128] * ga_ref[...]).astype(bf16)
    normed_b = (attend[:, 128:] * scale[:, 128:] * gb_ref[...]).astype(bf16)
    loads[0].wait()
    loads[1].wait()

    def project(yy):
        cols = pl.ds(pl.multiple_of(yy * 256, 256), 256)
        return dot(normed_a, pa[:, cols]) + dot(normed_b, pb[:, cols])

    mixed, to_mate1, to_chip1 = summed(project, p1s, p1o, p1v, p1r, p1i, p1ss, p1sr, p1rs, p1rr)
    first = depth_scale * res_ref[...].astype(f32) + mixed.astype(bf16).astype(f32)

    row8 = iota((8, 128), 0)

    def norm(n, total, gain, bias):
        sums = over_tp(n, rowsums(jnp.concatenate([total, total * total], axis=1)))
        mean = sums[0:1, :] / float(columns)
        var = sums[4:5, :] / float(columns) - mean * mean
        wide = spread(jnp.where(row8 < 4, mean, lax.rsqrt(var + norm_eps)), (0, 4), halves)
        return ((total - wide[:, :128]) * wide[:, 128:] * gain + bias).astype(bf16)

    settled = norm(1, first, gs_ref[...], bs_ref[...])

    def sp_copy(src, dst, send, recv, d):
        peer = lax.rem(sp + d, nsp)
        rows = pl.ds(pl.multiple_of(peer * STRIDE, STRIDE), STRIDE)
        here = pl.ds(pl.multiple_of(sp * STRIDE, STRIDE), STRIDE)
        return rcopy(src.at[rows, :], dst.at[here, :], send.at[d], recv.at[d], peer, tp)

    def sp_await(src, dst, send, recv, d):
        peer = lax.rem(sp - d + nsp, nsp)
        rows = pl.ds(pl.multiple_of(peer * STRIDE, STRIDE), STRIDE)
        rcopy(src.at[rows, :], dst.at[rows, :], send.at[d], recv.at[d], peer, tp).wait_recv()

    here = pl.ds(pl.multiple_of(sp * STRIDE, STRIDE), STRIDE)

    def exchange(src, dst, send, recv, value):
        src[...] = value
        loop(1, nsp, lambda d: sp_copy(src, dst, send, recv, d).start())
        dst[here, :] = src[here, :]
        loop(1, nsp, lambda d: sp_await(src, dst, send, recv, d))
        return dst[...]

    arrived = exchange(dsp, drv, ds_, dr_, dot_tl(choice[0] + choice[1], settled).astype(bf16))
    tokens = dot(compact, arrived).astype(bf16)

    side = pl.ds(pl.multiple_of(c * 128, 128), 128)
    mate_side = pl.ds(pl.multiple_of((1 - c) * 128, 128), 128)

    def to_same(d):
        block = xg.at[y, :, side]
        return rcopy(block, block, gs2.at[d], gr2.at[d], sp, lax.rem(y + d, ny) * 2 + c)

    def await_same(d):
        block = xg.at[lax.rem(y - d + ny, ny), :, side]
        rcopy(block, block, gs2.at[d], gr2.at[d], sp, lax.rem(y - d + ny, ny) * 2 + c).wait_recv()

    def hand_over(d):
        block = xg.at[lax.rem(y - d + ny, ny), :, side]
        return rcopy(block, block, fs2.at[d], fr2.at[d], sp, mate)

    def await_mate(d):
        block = xg.at[lax.rem(y - d + ny, ny), :, mate_side]
        rcopy(block, block, fs2.at[d], fr2.at[d], sp, mate).wait_recv()

    def take(d, start):
        yy = lax.rem(y - d + ny, ny)
        rows = pl.ds(pl.multiple_of(yy * 256, 256), 256)
        block = xg[yy]
        gate, up = dot(block, wg[rows, :]), dot(block, wu[rows, :])
        if start:
            acc_g[...] = gate
            acc_u[...] = up
        else:
            acc_g[...] += gate
            acc_u[...] += up

    xg[y, :, side] = tokens
    order = near_order(ny)
    hand_over(0).start()
    for d in order:
        to_same(d).start()
    loads[2].wait()
    loads[3].wait()
    before = 0
    for d in order:
        await_same(d)
        hand_over(d).start()
        await_mate(before)
        take(before, before == 0)
        before = d
    await_mate(before)
    take(before, False)

    gate = acc_g[...]
    hidden = (gate / (1.0 + jnp.exp(-gate)) * acc_u[...]).astype(bf16)
    loads[4].wait()

    def down(yy):
        return dot(hidden, wd[:, pl.ds(pl.multiple_of(yy * 256, 256), 256)])

    outputs, to_mate2, to_chip2 = summed(down, p2s, p2o, p2v, p2r, p2i, p2ss, p2sr, p2rs, p2rr)

    returned = exchange(rts, rtv, ts_, tr_, dot_tl(compact, outputs.astype(bf16)).astype(bf16))
    routed = route_ref[:, 0:1] * dot(choice[0], returned) + route_ref[:, 1:2] * dot(choice[1], returned)
    second = depth_scale * settled.astype(f32) + routed
    out_ref[...] = norm(2, second, gf_ref[...], bf_ref[...])

    for n in range(3):
        loop(1, ntp, lambda d, n=n: stat_copy(n, d).wait_send())
    for to_mate, to_chip in ((to_mate1, to_chip1), (to_mate2, to_chip2)):
        loop(0, ny, lambda d, f=to_mate: f(d).wait_send())
        loop(1, ny, lambda d, f=to_chip: f(d).wait_send())
    loop(1, nsp, lambda d: sp_copy(dsp, drv, ds_, dr_, d).wait_send())
    loop(1, nsp, lambda d: sp_copy(rts, rtv, ts_, tr_, d).wait_send())
    loop(1, ny, lambda d: to_same(d).wait_send())
    loop(0, ny, lambda d: hand_over(d).wait_send())


def body(
    nsp, ntp,
    residual_in, query_alpha, pairs_alpha, offset_alpha, gain_alpha,
    query_beta, pairs_beta, offset_beta, gain_beta, project_alpha, project_beta,
    gain_settle, bias_settle, expert_ids, route_weight,
    expert_gate, expert_up, expert_down, gain_final, bias_final,
):
    nz, ny = nsp // NX, ntp // 2
    vmem = pl.BlockSpec(memory_space=pltpu.VMEM)
    hbm = pl.BlockSpec(memory_space=pl.ANY)
    dma = pltpu.SemaphoreType.DMA
    V = pltpu.VMEM
    offsets = jnp.concatenate([offset_alpha.T, offset_beta.T, jnp.zeros((5, 128), f32)], axis=0)
    attend = pl.pallas_call(
        functools.partial(attend_kernel, nz),
        out_shape=jax.ShapeDtypeStruct((128, 256), f32),
        in_specs=[vmem] * 5,
        out_specs=vmem,
        scratch_shapes=[
            V((NX * 128, 128), bf16), V((NX * 128, 128), bf16), V((NX * 128, 256), bf16),
            V((8, NX * 128), f32), V((nz, 128, 128), bf16), V((nz, 128, 128), bf16),
            V((nz, 128, 256), bf16), V((nz, 128, 256), bf16), V((nz, 8, 128), f32), V((nz, 8, 128), f32),
            dma((3, NX)), dma((3, NX)), dma((2, nz)), dma((2, nz)), dma((2, nz)), dma((2, nz)),
        ],
        compiler_params=pltpu.CompilerParams(
            collective_id=0, has_side_effects=True, vmem_limit_bytes=32 * 1024 * 1024
        ),
        name="attend",
    )(query_alpha, query_beta, pairs_alpha.reshape(128, 128), pairs_beta.reshape(128, 256), offsets)

    rows = nsp * CAP
    wide = nsp * STRIDE

    def sum_scratch(height):
        return [
            V((ny, height, 128), bf16), V((ny, height, 128), f32), V((ny, height, 128), bf16),
            V((ny, height, 128), bf16), V((ny, height, 128), bf16),
            dma((ny,)), dma((ny,)), dma((ny,)), dma((ny,)),
        ]

    weights = (project_alpha, project_beta, expert_gate[0], expert_up[0], expert_down[0])
    vectors = [
        v.reshape(1, 128) for v in (gain_alpha, gain_beta, gain_settle, bias_settle, gain_final, bias_final)
    ]
    return pl.pallas_call(
        functools.partial(layer_kernel, nsp, ntp),
        out_shape=jax.ShapeDtypeStruct((128, 128), bf16),
        in_specs=[vmem] * 10 + [hbm] * 5,
        out_specs=vmem,
        scratch_shapes=[V(w.shape, bf16) for w in weights]
        + [dma((5,)), V((3, 8, 128), f32), V((3, ntp, 8, 128), f32), dma((3, ntp)), dma((3, ntp))]
        + sum_scratch(128)
        + [V((wide, 128), bf16), V((wide, 128), bf16), dma((nsp,)), dma((nsp,))]
        + [
            V((ny, rows, 256), bf16), dma((ny,)), dma((ny,)), dma((ny,)), dma((ny,)),
            V((rows, expert_gate.shape[2]), f32), V((rows, expert_gate.shape[2]), f32),
        ]
        + sum_scratch(rows)
        + [V((wide, 128), bf16), V((wide, 128), bf16), dma((nsp,)), dma((nsp,))],
        compiler_params=pltpu.CompilerParams(
            collective_id=1, has_side_effects=True, vmem_limit_bytes=48 * 1024 * 1024
        ),
        name="layer",
    )(attend, residual_in, *vectors, expert_ids, route_weight, *weights)


def solution(mesh):
    in_specs = (
        P("sp", "tp"),
        P("sp", "tp"),
        P("sp", "tp", None),
        P("sp", "tp"),
        P("tp"),
        P("sp", "tp"),
        P("sp", "tp", None),
        P("sp", "tp"),
        P("tp"),
        P("tp", None),
        P("tp", None),
        P("tp"),
        P("tp"),
        P("sp", None),
        P("sp", None),
        P("sp", None, "tp"),
        P("sp", None, "tp"),
        P("sp", "tp", None),
        P("tp"),
        P("tp"),
    )
    step = functools.partial(body, mesh.shape["sp"], mesh.shape["tp"])
    return jax.shard_map(step, mesh=mesh, in_specs=in_specs, out_specs=P("sp", "tp"), check_vma=False)
```

```python
import functools
import jax
import jax.numpy as jnp
from jax import lax
from jax.experimental import pallas as pl
from jax.experimental.pallas import tpu as pltpu
from jax.sharding import PartitionSpec as P

depth_scale = 2.0**0.5
norm_eps = 1e-05
MESH = pl.DeviceIdType.MESH
NX = 4
CAP = 12
STRIDE = 16
PIECES = 4
bf16 = jnp.bfloat16
f32 = jnp.float32


def iota(shape, dim):
    return lax.broadcasted_iota(jnp.int32, shape, dim)


def ones_where(cond):
    return jnp.where(cond, 1.0, 0.0).astype(bf16)


def dot(a, b):
    return jnp.dot(a, b, preferred_element_type=f32)


def dot_tr(a, b):
    return lax.dot_general(a, b, (((1,), (1,)), ((), ())), preferred_element_type=f32)


def dot_tl(a, b):
    return lax.dot_general(a, b, (((0,), (0,)), ((), ())), preferred_element_type=f32)


def split(v, pieces):
    found = []
    for _ in range(pieces):
        part = v.astype(bf16)
        found.append(part)
        v = v - part.astype(f32)
    return found


def spread(rows8, low, high):
    parts = [p.astype(f32) for p in split(rows8, 3)] + [jnp.zeros_like(rows8)]
    stacked = jnp.concatenate(parts, axis=0).astype(bf16)
    row = iota((32, 256), 0)
    lane = iota((32, 256), 1)
    slot = row & 7
    pick = jnp.zeros((32, 256), jnp.bool_)
    for r, (first, last) in zip(low, high):
        pick = pick | ((slot == r) & (lane >= first) & (lane < last) & (row < 24))
    return dot_tl(stacked, ones_where(pick))


def rowsums(v):
    cat = jnp.concatenate(split(v, 3), axis=1)
    lane = iota((8, 768), 1) & 255
    row = iota((8, 768), 0)
    return dot_tr(ones_where((lane < 128) == (row < 4)), cat)


def rcopy(src, dst, send, recv, sp, tp):
    return pltpu.make_async_remote_copy(
        src_ref=src, dst_ref=dst, send_sem=send, recv_sem=recv, device_id=(sp, tp), device_id_type=MESH
    )


def loop(low, high, step):
    def run(i, carry):
        step(i)
        return carry

    lax.fori_loop(low, high, run, 0)


def near_order(n):
    return sorted(range(1, n), key=lambda d: (min(d, n - d), d))


def layer_kernel(
    nsp, ntp,
    qa_ref, qb_ref, ka_ref, kb_ref, oa_ref, ob_ref, res_ref, ga_ref, gb_ref, gs_ref, bs_ref, gf_ref, bf_ref,
    ids_ref, route_ref, pa_hbm, pb_hbm, wg_hbm, wu_hbm, wd_hbm, out_ref,
    pa, pb, wg, wu, wd, wsem, misc,
    kva, kvr, kvb, ofs, off, qba, qbb, ret, back, tot, tback,
    ks, kr, qs, qr, rs, rr,
    stat, stats, ss, sr,
    p1s, p1o, p1v, p1r, p1i, p1ss, p1sr, p1rs, p1rr,
    dsp, drv, ds_, dr_,
    xg, as_, ar_, hs_, hr_, acc_g, acc_u,
    p2s, p2o, p2v, p2ss, p2sr, rb_s, rb_r, rbs_, rbr_,
    rts, rtv, ts_, tr_,
):
    sp, tp = lax.axis_index("sp"), lax.axis_index("tp")
    nz, ny = nsp // NX, ntp // 2
    z, x = lax.div(sp, NX), lax.rem(sp, NX)
    y, c = lax.div(tp, 2), lax.rem(tp, 2)
    mate = y * 2 + 1 - c
    columns = ntp * 128
    ends = []

    loads = [
        pltpu.make_async_copy(src, dst, wsem.at[i])
        for i, (src, dst) in enumerate(
            ((pa_hbm, pa), (pb_hbm, pb), (wg_hbm, wg), (wu_hbm, wu), (wd_hbm, wd))
        )
    ]
    for load in loads:
        load.start()

    barrier = pltpu.get_barrier_semaphore()

    def greet_sp(d):
        pl.semaphore_signal(barrier, 1, device_id=(lax.rem(sp + d, nsp), tp), device_id_type=MESH)

    def greet_tp(d):
        pl.semaphore_signal(barrier, 1, device_id=(sp, lax.rem(tp + d, ntp)), device_id_type=MESH)

    loop(1, nsp, greet_sp)
    loop(1, ntp, greet_tp)
    ofs[...] = jnp.zeros((8, 128), f32)
    ofs[0:2, :] = oa_ref[...]
    ofs[2:3, :] = ob_ref[...]
    pl.semaphore_wait(barrier, nsp - 1 + ntp - 1)

    def key_copies(d, src_x):
        peer = z * NX + lax.rem(x + d, NX)
        rows = pl.ds(pl.multiple_of(src_x * 128, 128), 128)
        return (
            rcopy(ka_ref, kva.at[rows, :], ks.at[0, d], kr.at[0, d], peer, tp),
            rcopy(kb_ref, kvb.at[rows, :], ks.at[1, d], kr.at[1, d], peer, tp),
            rcopy(ofs, off.at[:, rows], ks.at[2, d], kr.at[2, d], peer, tp),
        )

    def query_copies(dst_z, src_z):
        peer = dst_z * NX + x
        return (
            rcopy(qa_ref, qba.at[src_z], qs.at[0, dst_z], qr.at[0, src_z], peer, tp),
            rcopy(qb_ref, qbb.at[src_z], qs.at[1, dst_z], qr.at[1, src_z], peer, tp),
        )

    def result_copies(dst_z, src_z):
        peer = dst_z * NX + x
        return (
            rcopy(ret.at[dst_z], back.at[src_z], rs.at[0, dst_z], rr.at[0, src_z], peer, tp),
            rcopy(tot.at[dst_z], tback.at[src_z], rs.at[1, dst_z], rr.at[1, src_z], peer, tp),
        )

    def send_keys(d):
        for copy in key_copies(d, x):
            copy.start()

    loop(1, NX, send_keys)

    def send_query(k):
        for copy in query_copies(z - 1 - k, z):
            copy.start()

    loop(0, z, send_query)

    mine = pl.ds(pl.multiple_of(x * 128, 128), 128)
    kva[mine, :] = ka_ref[...]
    kvb[mine, :] = kb_ref[...]
    off[:, mine] = ofs[...]
    qba[z] = qa_ref[...]
    qbb[z] = qb_ref[...]

    def await_keys(d):
        for copy in key_copies(d, lax.rem(x - d + NX, NX)):
            copy.wait_recv()

    loop(1, NX, await_keys)
    keys_a = kva[...]
    kvr[...] = pltpu.roll(keys_a.astype(f32), 64, 1).astype(bf16)

    lane = iota((128, 128), 1)
    gap = lane - iota((128, 128), 0)
    r256, c256 = iota((256, 256), 0) & 127, iota((256, 256), 1)
    later_matrix = ones_where((r256 > c256) | (c256 >= 128))
    ones8 = jnp.ones((8, 256), bf16)
    row8 = iota((8, 128), 0)

    def visit(zq):
        @pl.when(zq > z)
        def _():
            for copy in query_copies(z, zq):
                copy.wait_recv()

        qa, qb = qba[zq], qbb[zq]
        zero = jnp.zeros_like(qa)
        accs, totals = [], []
        for h in range(3):
            q = (jnp.where(lane < 64, qa, zero), jnp.where(lane >= 64, qa, zero), qb)[h]
            scale = (64.0**-0.5, 64.0**-0.5, 128.0**-0.5)[h]
            gone = jnp.zeros((128, 128), f32)
            total = jnp.zeros((8, 128), f32)
            weights = [None] * NX
            for b in reversed(range(NX)):
                rows = slice(b * 128, b * 128 + 128)
                keys = (kva[rows, :], kvr[rows, :], kvb[rows, :128])[h]
                scores = dot_tr(q, keys) * scale + off[h : h + 1, rows]
                valid = gap < (zq - z) * (NX * 128) + (x - b) * 128
                soft = jnp.maximum(scores, 0.0) + jnp.log(1.0 + jnp.exp(-jnp.abs(scores)))
                cat = jnp.concatenate(split(jnp.where(valid, soft, 0.0), 2), axis=1)
                sums = dot(cat, later_matrix)
                total = total + dot_tr(ones8, cat)
                power = (scores - soft) - (sums[:, :128] + gone)
                gone = gone + sums[:, 128:]
                weights[b] = jnp.where(valid, jnp.exp(power), 0.0).astype(bf16)
            values = (kvr[...], kva[...], kvb[:, 128:])[h]
            accs.append(dot(jnp.concatenate(weights, axis=1), values))
            totals.append(total)
        both = jnp.where(lane < 64, accs[0], accs[1])
        found = jnp.concatenate([both, accs[2]], axis=1).astype(bf16)
        sums8 = jnp.where(row8 == 0, totals[0], jnp.where(row8 == 1, totals[1], totals[2]))

        @pl.when(zq == z)
        def _():
            back[z] = found
            tback[z] = sums8

        @pl.when(zq > z)
        def _():
            ret[zq] = found
            tot[zq] = sums8
            for copy in result_copies(zq, z):
                copy.start()

    loop(z, nz, visit)

    def gather(k, carry):
        acc, gone = carry
        zk = z - k

        @pl.when(k > 0)
        def _():
            for copy in result_copies(z, zk):
                copy.wait_recv()

        wide = spread(jnp.exp(-gone), (0, 1, 2), ((0, 64), (64, 128), (128, 256)))
        return acc + wide * back[zk].astype(f32), gone + tback[zk]

    attend, _ = lax.fori_loop(
        0, z + 1, gather, (jnp.zeros((128, 256), f32), jnp.zeros((8, 128), f32))
    )

    def end_attend():
        def end_keys(d):
            for copy in key_copies(d, x):
                copy.wait_send()

        def end_query(k):
            for copy in query_copies(z - 1 - k, z):
                copy.wait_send()

        def end_result(zq):
            for copy in result_copies(zq, z):
                copy.wait_send()

        loop(1, NX, end_keys)
        loop(0, z, end_query)
        loop(z + 1, nz, end_result)

    ends.append(end_attend)

    def stat_copy(n, d):
        return rcopy(stat.at[n], stats.at[n, d], ss.at[n, d], sr.at[n, d], sp, lax.rem(tp + d, ntp))

    def over_tp(n, rows8):
        stat[n] = rows8
        loop(1, ntp, lambda d: stat_copy(n, d).start())
        ends.append(lambda: loop(1, ntp, lambda d: stat_copy(n, d).wait_send()))
        loop(1, ntp, lambda d: stat_copy(n, d).wait_recv())
        total = rows8
        for d in range(1, ntp):
            total = total + stats[n, d]
        return total

    def halves_of(both):
        left, right = both[:, :128], both[:, 128:]
        return jnp.where(c == 0, left, right), jnp.where(c == 0, right, left)

    halves = ((0, 128), (128, 256))
    misc[...] = jnp.zeros((8, 128), f32)
    misc[0:2, :] = ids_ref[...].astype(f32)
    misc[2:4, :] = route_ref[...]
    facts = misc[...]
    id_cols = spread(facts, (0, 1), halves)
    route_cols = spread(facts, (2, 3), halves)
    lane128 = iota((128, 128), 1)
    lane_f = lane128.astype(f32)
    id_col = (id_cols[:, :128], id_cols[:, 128:])
    hot = [v == lane_f for v in id_col]
    tri = ones_where(iota((128, 128), 0) > lane128)
    earlier = dot(tri, ones_where(hot[0] | hot[1]))
    lane_all = iota((128, nsp * STRIDE), 1).astype(f32)
    choice = []
    for k in range(2):
        slot = jnp.sum(jnp.where(hot[k], earlier, 0.0), axis=1, keepdims=True)
        place = id_col[k][:, :1] * float(STRIDE) + slot
        choice.append(ones_where(place == lane_all))
    row_c, col_c = iota((nsp * CAP, nsp * STRIDE), 0), iota((nsp * CAP, nsp * STRIDE), 1)
    block_c = (row_c * (-(-(1 << 17) // CAP))) >> 17
    compact = ones_where(col_c == row_c + block_c * (STRIDE - CAP))

    squares = over_tp(0, rowsums(attend * attend))
    scale = spread(lax.rsqrt(squares / float(columns) + norm_eps), (0, 4), halves)
    normed_a = (attend[:, :128] * scale[:, :128] * ga_ref[...]).astype(bf16)
    normed_b = (attend[:, 128:] * scale[:, 128:] * gb_ref[...]).astype(bf16)
    loads[0].wait()
    loads[1].wait()

    def project(yy):
        cols = pl.ds(pl.multiple_of(yy * 256, 256), 256)
        return dot(normed_a, pa[:, cols]) + dot(normed_b, pb[:, cols])

    def mate1(d):
        return rcopy(p1s.at[d], p1v.at[d], p1ss.at[d], p1sr.at[d], sp, mate)

    def chip1(d):
        return rcopy(p1r.at[d], p1i.at[d], p1rs.at[d], p1rr.at[d], sp, lax.rem(y + d, ny) * 2 + c)

    def make1(d):
        own, other = halves_of(project(lax.rem(y + d, ny)))
        p1s[d] = other.astype(bf16)
        mate1(d).start()
        p1o[d] = own

    def pass1(d):
        mate1(d).wait_recv()
        p1r[d] = (p1o[d] + p1v[d].astype(f32)).astype(bf16)
        chip1(d).start()

    order = near_order(ny)[::-1]
    make1(order[0])
    for before, d in zip(order, order[1:] + [0]):
        make1(d)
        pass1(before)
    mate1(0).wait_recv()
    mixed = p1o[0] + p1v[0].astype(f32)
    for d in order[::-1]:
        chip1(d).wait_recv()
        mixed = mixed + p1i[d].astype(f32)
    ends.append(lambda: loop(0, ny, lambda d: mate1(d).wait_send()))
    ends.append(lambda: loop(1, ny, lambda d: chip1(d).wait_send()))
    first = depth_scale * res_ref[...].astype(f32) + mixed.astype(bf16).astype(f32)

    def norm(n, total, gain, bias):
        sums = over_tp(n, rowsums(jnp.concatenate([total, total * total], axis=1)))
        mean = sums[0:1, :] / float(columns)
        var = sums[4:5, :] / float(columns) - mean * mean
        wide = spread(jnp.where(row8 < 4, mean, lax.rsqrt(var + norm_eps)), (0, 4), halves)
        return ((total - wide[:, :128]) * wide[:, 128:] * gain + bias).astype(bf16)

    settled = norm(1, first, gs_ref[...], bs_ref[...])

    here = pl.ds(pl.multiple_of(sp * STRIDE, STRIDE), STRIDE)

    def sp_copy(src, dst, send, recv, d):
        peer = lax.rem(sp + d, nsp)
        rows = pl.ds(pl.multiple_of(peer * STRIDE, STRIDE), STRIDE)
        return rcopy(src.at[rows, :], dst.at[here, :], send.at[d], recv.at[d], peer, tp)

    def sp_await(src, dst, send, recv, d):
        peer = lax.rem(sp - d + nsp, nsp)
        rows = pl.ds(pl.multiple_of(peer * STRIDE, STRIDE), STRIDE)
        rcopy(src.at[rows, :], dst.at[rows, :], send.at[d], recv.at[d], peer, tp).wait_recv()

    def exchange(src, dst, send, recv, value):
        src[...] = value
        loop(1, nsp, lambda d: sp_copy(src, dst, send, recv, d).start())
        ends.append(lambda: loop(1, nsp, lambda d: sp_copy(src, dst, send, recv, d).wait_send()))
        dst[here, :] = src[here, :]
        loop(1, nsp, lambda d: sp_await(src, dst, send, recv, d))
        return dst[...]

    arrived = exchange(dsp, drv, ds_, dr_, dot_tl(choice[0] + choice[1], settled).astype(bf16))
    tokens = dot(compact, arrived).astype(bf16)

    half = ny // 2
    height = nsp * CAP // PIECES
    ways = (0, 1)

    def chip_at(steps):
        return lax.rem(y + steps + ny, ny)

    def last_hop(way, p):
        return half if (p < PIECES // 2) == (way == 0) else half - 1

    def block_of(way, hop, core):
        source = chip_at(-hop if way == 0 else hop)
        return source, pl.ds(pl.multiple_of(core * 128, 128), 128)

    def along(way, hop, p):
        source, side = block_of(way, hop, c)
        block = xg.at[source, pl.ds(p * height, height), side]
        target = chip_at(1 if way == 0 else -1) * 2 + c
        return rcopy(block, block, as_.at[way, hop, p], ar_.at[way, hop + 1, p], sp, target)

    def along_await(way, hop, p):
        source, side = block_of(way, hop, c)
        block = xg.at[source, pl.ds(p * height, height), side]
        target = chip_at(-1 if way == 0 else 1) * 2 + c
        rcopy(block, block, as_.at[way, hop, p], ar_.at[way, hop, p], sp, target).wait_recv()

    def across(way, hop, p):
        source, side = block_of(way, hop, c)
        block = xg.at[source, pl.ds(p * height, height), side]
        return rcopy(block, block, hs_.at[way, hop, p], hr_.at[way, hop, p], sp, mate)

    def across_await(way, hop, p):
        source, side = block_of(way, hop, 1 - c)
        block = xg.at[source, pl.ds(p * height, height), side]
        rcopy(block, block, hs_.at[way, hop, p], hr_.at[way, hop, p], sp, mate).wait_recv()

    def take(source, start):
        rows = pl.ds(pl.multiple_of(source * 256, 256), 256)
        block = xg[source]
        gate, up = dot(block, wg[rows, :]), dot(block, wu[rows, :])
        if start:
            acc_g[...] = gate
            acc_u[...] = up
        else:
            acc_g[...] += gate
            acc_u[...] += up

    xg[y, :, pl.ds(pl.multiple_of(c * 128, 128), 128)] = tokens
    sends = [(way, 0, p) for p in range(PIECES) for way in ways if last_hop(way, p) > 0]
    crossings = [(0, 0, p) for p in range(PIECES)]
    for key in sends:
        along(*key).start()
    for key in crossings:
        across(*key).start()
    loads[2].wait()
    loads[3].wait()
    for p in range(PIECES):
        across_await(0, 0, p)
    take(y, True)
    for hop in range(1, half + 1):
        reached = [(way, hop, p) for p in range(PIECES) for way in ways if hop <= last_hop(way, p)]
        for key in reached:
            way, _, p = key
            along_await(*key)
            if hop < last_hop(way, p):
                along(*key).start()
                sends.append(key)
            across(*key).start()
            crossings.append(key)
        for key in reached:
            across_await(*key)
        take(chip_at(-hop), False)
        if hop < half:
            take(chip_at(hop), False)

    def end_gather():
        for key in sends:
            along(*key).wait_send()
        for key in crossings:
            across(*key).wait_send()

    ends.append(end_gather)

    gate = acc_g[...]
    hidden = (gate / (1.0 + jnp.exp(-gate)) * acc_u[...]).astype(bf16)
    loads[4].wait()

    def mate2(d):
        return rcopy(p2s.at[d], p2v.at[d], p2ss.at[d], p2sr.at[d], sp, mate)

    def make2(d):
        cols = pl.ds(pl.multiple_of(lax.rem(y + d, ny) * 256, 256), 256)
        own, other = halves_of(dot(hidden, wd[:, cols]))
        p2s[d] = other.astype(bf16)
        mate2(d).start()
        p2o[d] = own

    def term2(d, p):
        rows = slice(p * height, p * height + height)
        return p2o[d, rows, :] + p2v[d, rows, :].astype(f32)

    def pass2(way, step, p):
        rows = pl.ds(p * height, height)
        target = chip_at(1 if way == 0 else -1) * 2 + c
        return rcopy(
            rb_s.at[way, step, rows, :], rb_r.at[way, step, rows, :],
            rbs_.at[way, step, p], rbr_.at[way, step, p], sp, target,
        )

    passes = []

    def hand_on(step):
        left = half - step
        for p in range(PIECES):
            for way in ways:
                start = half - last_hop(way, p)
                if step < start:
                    continue
                rows = slice(p * height, p * height + height)
                value = term2(left if way == 0 else ny - left, p)
                if step > start:
                    pass2(way, step - 1, p).wait_recv()
                    value = value + rb_r[way, step - 1, rows, :].astype(f32)
                rb_s[way, step, rows, :] = value.astype(bf16)
                pass2(way, step, p).start()
                passes.append((way, step, p))

    make2(half)
    for step in range(half):
        left = half - step
        if left > 1:
            make2(left - 1)
            make2(ny - left + 1)
        else:
            make2(0)
        mate2(left).wait_recv()
        if left < half:
            mate2(ny - left).wait_recv()
        hand_on(step)
    mate2(0).wait_recv()
    outputs = []
    for p in range(PIECES):
        rows = slice(p * height, p * height + height)
        value = term2(0, p)
        for way in ways:
            if last_hop(way, p) > 0:
                pass2(way, half - 1, p).wait_recv()
                value = value + rb_r[way, half - 1, rows, :].astype(f32)
        outputs.append(value.astype(bf16))

    def end_sum():
        loop(0, ny, lambda d: mate2(d).wait_send())
        for key in passes:
            pass2(*key).wait_send()

    ends.append(end_sum)
    outputs = jnp.concatenate(outputs, axis=0)

    returned = exchange(rts, rtv, ts_, tr_, dot_tl(compact, outputs).astype(bf16))
    routed = route_cols[:, :128] * dot(choice[0], returned) + route_cols[:, 128:] * dot(choice[1], returned)
    second = depth_scale * settled.astype(f32) + routed
    out_ref[...] = norm(2, second, gf_ref[...], bf_ref[...])
    for end in ends:
        end()


def body(
    nsp, ntp,
    residual_in, query_alpha, pairs_alpha, offset_alpha, gain_alpha,
    query_beta, pairs_beta, offset_beta, gain_beta, project_alpha, project_beta,
    gain_settle, bias_settle, expert_ids, route_weight,
    expert_gate, expert_up, expert_down, gain_final, bias_final,
):
    nz, ny = nsp // NX, ntp // 2
    vmem = pl.BlockSpec(memory_space=pltpu.VMEM)
    hbm = pl.BlockSpec(memory_space=pl.ANY)
    dma = pltpu.SemaphoreType.DMA
    V = pltpu.VMEM
    rows = nsp * CAP
    wide = nsp * STRIDE
    half = ny // 2
    weights = (project_alpha, project_beta, expert_gate[0], expert_up[0], expert_down[0])
    vectors = [
        v.reshape(1, 128) for v in (gain_alpha, gain_beta, gain_settle, bias_settle, gain_final, bias_final)
    ]
    scratch = [V(w.shape, bf16) for w in weights] + [dma((5,)), V((8, 128), f32)]
    scratch += [
        V((NX * 128, 128), bf16), V((NX * 128, 128), bf16), V((NX * 128, 256), bf16),
        V((8, 128), f32), V((8, NX * 128), f32), V((nz, 128, 128), bf16), V((nz, 128, 128), bf16),
        V((nz, 128, 256), bf16), V((nz, 128, 256), bf16), V((nz, 8, 128), f32), V((nz, 8, 128), f32),
        dma((3, NX)), dma((3, NX)), dma((2, nz)), dma((2, nz)), dma((2, nz)), dma((2, nz)),
    ]
    scratch += [V((3, 8, 128), f32), V((3, ntp, 8, 128), f32), dma((3, ntp)), dma((3, ntp))]
    scratch += [
        V((ny, 128, 128), bf16), V((ny, 128, 128), f32), V((ny, 128, 128), bf16),
        V((ny, 128, 128), bf16), V((ny, 128, 128), bf16), dma((ny,)), dma((ny,)), dma((ny,)), dma((ny,)),
    ]
    scratch += [V((wide, 128), bf16), V((wide, 128), bf16), dma((nsp,)), dma((nsp,))]
    hops = (2, half + 1, PIECES)
    scratch += [
        V((ny, rows, 256), bf16), dma(hops), dma(hops), dma(hops), dma(hops),
        V((rows, expert_gate.shape[2]), f32), V((rows, expert_gate.shape[2]), f32),
    ]
    scratch += [
        V((ny, rows, 128), bf16), V((ny, rows, 128), f32), V((ny, rows, 128), bf16), dma((ny,)), dma((ny,)),
        V((2, half, rows, 128), bf16), V((2, half, rows, 128), bf16), dma(hops), dma(hops),
    ]
    scratch += [V((wide, 128), bf16), V((wide, 128), bf16), dma((nsp,)), dma((nsp,))]
    return pl.pallas_call(
        functools.partial(layer_kernel, nsp, ntp),
        out_shape=jax.ShapeDtypeStruct((128, 128), bf16),
        in_specs=[vmem] * 15 + [hbm] * 5,
        out_specs=vmem,
        scratch_shapes=scratch,
        compiler_params=pltpu.CompilerParams(
            collective_id=0, has_side_effects=True, vmem_limit_bytes=62 * 1024 * 1024
        ),
        name="layer",
    )(
        query_alpha, query_beta, pairs_alpha.reshape(128, 128), pairs_beta.reshape(128, 256),
        offset_alpha.T, offset_beta.T, residual_in, *vectors, expert_ids.T, route_weight.T, *weights,
    )


def solution(mesh):
    in_specs = (
        P("sp", "tp"),
        P("sp", "tp"),
        P("sp", "tp", None),
        P("sp", "tp"),
        P("tp"),
        P("sp", "tp"),
        P("sp", "tp", None),
        P("sp", "tp"),
        P("tp"),
        P("tp", None),
        P("tp", None),
        P("tp"),
        P("tp"),
        P("sp", None),
        P("sp", None),
        P("sp", None, "tp"),
        P("sp", None, "tp"),
        P("sp", "tp", None),
        P("tp"),
        P("tp"),
    )
    step = functools.partial(body, mesh.shape["sp"], mesh.shape["tp"])
    return jax.shard_map(step, mesh=mesh, in_specs=in_specs, out_specs=P("sp", "tp"), check_vma=False)
```

```python
import functools
import jax
import jax.numpy as jnp
from jax import lax
from jax.experimental import pallas as pl
from jax.experimental.pallas import tpu as pltpu
from jax.sharding import PartitionSpec as P

depth_scale = 2.0**0.5
norm_eps = 1e-05
MESH = pl.DeviceIdType.MESH
NX = 4
CAP = 12
STRIDE = 16
PIECES = 4
PLANES = 2
bf16 = jnp.bfloat16
f32 = jnp.float32


def iota(shape, dim):
    return lax.broadcasted_iota(jnp.int32, shape, dim)


def ones_where(cond):
    return jnp.where(cond, 1.0, 0.0).astype(bf16)


def dot(a, b):
    return jnp.dot(a, b, preferred_element_type=f32)


def dot_tr(a, b):
    return lax.dot_general(a, b, (((1,), (1,)), ((), ())), preferred_element_type=f32)


def dot_tl(a, b):
    return lax.dot_general(a, b, (((0,), (0,)), ((), ())), preferred_element_type=f32)


def split(v, pieces):
    found = []
    for _ in range(pieces):
        part = v.astype(bf16)
        found.append(part)
        v = v - part.astype(f32)
    return found


def spread(rows8, low, high):
    parts = [p.astype(f32) for p in split(rows8, 3)] + [jnp.zeros_like(rows8)]
    stacked = jnp.concatenate(parts, axis=0).astype(bf16)
    row = iota((32, 256), 0)
    lane = iota((32, 256), 1)
    slot = row & 7
    pick = jnp.zeros((32, 256), jnp.bool_)
    for r, (first, last) in zip(low, high):
        pick = pick | ((slot == r) & (lane >= first) & (lane < last) & (row < 24))
    return dot_tl(stacked, ones_where(pick))


def rowsums(v):
    cat = jnp.concatenate(split(v, 3), axis=1)
    lane = iota((8, 768), 1) & 255
    row = iota((8, 768), 0)
    return dot_tr(ones_where((lane < 128) == (row < 4)), cat)


def rcopy(src, dst, send, recv, sp, tp):
    return pltpu.make_async_remote_copy(
        src_ref=src, dst_ref=dst, send_sem=send, recv_sem=recv, device_id=(sp, tp), device_id_type=MESH
    )


def loop(low, high, step):
    def run(i, carry):
        step(i)
        return carry

    lax.fori_loop(low, high, run, 0)


def near_order(n):
    return sorted(range(1, n), key=lambda d: (min(d, n - d), d))


def layer_kernel(
    nsp, ntp,
    qa_ref, qb_ref, ka_ref, kb_ref, oa_ref, ob_ref, res_ref, ga_ref, gb_ref, gs_ref, bs_ref, gf_ref, bf_ref,
    ids_ref, route_ref, pa_hbm, pb_hbm, wg_hbm, wu_hbm, wd_hbm, out_ref,
    pa, pb, wg, wu, wd, wsem, misc,
    kva, kvr, kvb, ofs, off, qba, qbb, ret, back, tot, tback,
    ks, kr, qs, qr, rs, rr,
    vec, vecs, vs_, vr_, mr, ssp, srv, ds2, dr2,
    stat, stats, ss, sr,
    p1s, p1o, p1v, p1r, p1i, p1ss, p1sr, p1rs, p1rr,
    dsp, drv, ds_, dr_,
    xg, as_, ar_, hs_, hr_, acc_g, acc_u,
    p2s, p2o, p2v, p2ss, p2sr, rb_s, rb_r, rbs_, rbr_,
    rts, rtv, ts_, tr_,
):
    sp, tp = lax.axis_index("sp"), lax.axis_index("tp")
    nz, ny = nsp // NX, ntp // 2
    z, x = lax.div(sp, NX), lax.rem(sp, NX)
    y, c = lax.div(tp, 2), lax.rem(tp, 2)
    mate = y * 2 + 1 - c
    columns = ntp * 128
    ends = []

    loads = [
        pltpu.make_async_copy(src, dst, wsem.at[i])
        for i, (src, dst) in enumerate(
            ((pa_hbm, pa), (pb_hbm, pb), (wg_hbm, wg), (wu_hbm, wu), (wd_hbm, wd))
        )
    ]
    for load in loads:
        load.start()

    barrier = pltpu.get_barrier_semaphore()

    def greet_sp(d):
        pl.semaphore_signal(barrier, 1, device_id=(lax.rem(sp + d, nsp), tp), device_id_type=MESH)

    def greet_tp(d):
        pl.semaphore_signal(barrier, 1, device_id=(sp, lax.rem(tp + d, ntp)), device_id_type=MESH)

    loop(1, nsp, greet_sp)
    loop(1, ntp, greet_tp)
    ofs[...] = jnp.zeros((8, 128), f32)
    ofs[0:2, :] = oa_ref[...]
    ofs[2:3, :] = ob_ref[...]
    vec[...] = jnp.zeros((8, 128), f32)
    vec[0:1, :] = gs_ref[...]
    vec[1:2, :] = bs_ref[...]
    pl.semaphore_wait(barrier, nsp - 1 + ntp - 1)

    groups = nz // PLANES
    zp, zb = lax.div(z, PLANES), lax.rem(z, PLANES)
    other_z = z + 1 - 2 * zb
    here_slot, there_slot = zb * NX, (1 - zb) * NX

    def key_copies(passed, k, slot, peer):
        rows = pl.ds(pl.multiple_of(slot * 128, 128), 128)
        sources = (kva.at[rows, :], kvb.at[rows, :], off.at[:, rows]) if passed else (ka_ref, kb_ref, ofs)
        targets = (kva.at[rows, :], kvb.at[rows, :], off.at[:, rows])
        return [
            rcopy(src, dst, ks.at[i, k], kr.at[i, k], peer, tp)
            for i, (src, dst) in enumerate(zip(sources, targets))
        ]

    def x_peer(d):
        return z * NX + lax.rem(x + d, NX)

    def cross_copies(slot):
        return key_copies(False, 0, slot + x, other_z * NX + x)

    def query_copies(dst_z, src_z):
        peer = dst_z * NX + x
        return (
            rcopy(qa_ref, qba.at[src_z], qs.at[0, dst_z], qr.at[0, src_z], peer, tp),
            rcopy(qb_ref, qbb.at[src_z], qs.at[1, dst_z], qr.at[1, src_z], peer, tp),
        )

    def result_copies(dst_z, src_z):
        peer = dst_z * NX + x
        return (
            rcopy(ret.at[dst_z], back.at[src_z], rs.at[0, dst_z], rr.at[0, src_z], peer, tp),
            rcopy(tot.at[dst_z], tback.at[src_z], rs.at[1, dst_z], rr.at[1, src_z], peer, tp),
        )

    for copy in cross_copies(here_slot):
        copy.start()

    def send_keys(d):
        for copy in key_copies(False, d, here_slot + x, x_peer(d)):
            copy.start()

    loop(1, NX, send_keys)

    def send_query(k):
        for copy in query_copies(z - PLANES * (k + 1), z):
            copy.start()

    loop(0, zp, send_query)

    def vec_copy(d):
        return rcopy(vec, vecs.at[tp], vs_.at[d], vr_.at[d], sp, lax.rem(tp + d, ntp))

    def vec_await(d):
        source = lax.rem(tp - d + ntp, ntp)
        rcopy(vec, vecs.at[source], vs_.at[d], vr_.at[d], sp, source).wait_recv()

    loop(1, ntp, lambda d: vec_copy(d).start())
    ends.append(lambda: loop(1, ntp, lambda d: vec_copy(d).wait_send()))
    vecs[tp] = vec[...]

    mine = pl.ds(pl.multiple_of((here_slot + x) * 128, 128), 128)
    kva[mine, :] = ka_ref[...]
    kvb[mine, :] = kb_ref[...]
    off[:, mine] = ofs[...]
    qba[z] = qa_ref[...]
    qbb[z] = qb_ref[...]

    for copy in cross_copies(there_slot):
        copy.wait_recv()

    def pass_keys(d):
        for copy in key_copies(True, NX + d, there_slot + x, x_peer(d)):
            copy.start()

    loop(1, NX, pass_keys)

    def await_keys(d):
        source = lax.rem(x - d + NX, NX)
        for copy in key_copies(False, d, here_slot + source, x_peer(d)):
            copy.wait_recv()
        for copy in key_copies(True, NX + d, there_slot + source, x_peer(d)):
            copy.wait_recv()

    loop(1, NX, await_keys)
    keys_a = kva[...]
    kvr[...] = pltpu.roll(keys_a.astype(f32), 64, 1).astype(bf16)

    lane = iota((128, 128), 1)
    gap = lane - iota((128, 128), 0)
    r256, c256 = iota((256, 256), 0) & 127, iota((256, 256), 1)
    later_matrix = ones_where((r256 > c256) | (c256 >= 128))
    first_lane = ones_where((iota((8, 384), 1) & 127) == 0)
    row8 = iota((8, 128), 0)

    def visit(m):
        zq = z + PLANES * m

        @pl.when(zq > z)
        def _():
            for copy in query_copies(z, zq):
                copy.wait_recv()

        qa, qb = qba[zq], qbb[zq]
        zero = jnp.zeros_like(qa)
        accs, totals = [], []
        for h in range(3):
            q = (jnp.where(lane < 64, qa, zero), jnp.where(lane >= 64, qa, zero), qb)[h]
            scale = (64.0**-0.5, 64.0**-0.5, 128.0**-0.5)[h]
            gone = jnp.zeros((128, 128), f32)
            weights = [None] * (PLANES * NX)
            for b in reversed(range(PLANES * NX)):
                rows = slice(b * 128, b * 128 + 128)
                keys = (kva[rows, :], kvr[rows, :], kvb[rows, :128])[h]
                scores = dot_tr(q, keys) * scale + off[h : h + 1, rows]
                valid = gap < ((zq - zp * PLANES) * NX + x - b) * 128
                soft = jnp.maximum(scores, 0.0) + jnp.log(1.0 + jnp.exp(-jnp.abs(scores)))
                cat = jnp.concatenate(split(jnp.where(valid, soft, 0.0), 2), axis=1)
                sums = dot(cat, later_matrix)
                power = (scores - soft) - (sums[:, :128] + gone)
                gone = gone + sums[:, 128:]
                weights[b] = jnp.where(valid, jnp.exp(power), 0.0).astype(bf16)
            values = (kvr[...], kva[...], kvb[:, 128:])[h]
            accs.append(dot(jnp.concatenate(weights, axis=1), values))
            totals.append(dot_tr(first_lane, jnp.concatenate(split(gone, 3), axis=1)))
        both = jnp.where(lane < 64, accs[0], accs[1])
        found = jnp.concatenate([both, accs[2]], axis=1).astype(bf16)
        sums8 = jnp.where(row8 == 0, totals[0], jnp.where(row8 == 1, totals[1], totals[2]))

        @pl.when(zq == z)
        def _():
            back[z] = found
            tback[z] = sums8

        @pl.when(zq > z)
        def _():
            ret[zq] = found
            tot[zq] = sums8
            for copy in result_copies(zq, z):
                copy.start()

    loop(0, groups - zp, visit)

    def gather(k, carry):
        acc, gone = carry
        zk = z - PLANES * k

        @pl.when(k > 0)
        def _():
            for copy in result_copies(z, zk):
                copy.wait_recv()

        wide = spread(jnp.exp(-gone), (0, 1, 2), ((0, 64), (64, 128), (128, 256)))
        return acc + wide * back[zk].astype(f32), gone + tback[zk]

    attend, _ = lax.fori_loop(
        0, zp + 1, gather, (jnp.zeros((128, 256), f32), jnp.zeros((8, 128), f32))
    )

    def end_attend():
        for copy in cross_copies(here_slot):
            copy.wait_send()

        def end_keys(d):
            for copy in key_copies(False, d, here_slot + x, x_peer(d)):
                copy.wait_send()
            for copy in key_copies(True, NX + d, there_slot + x, x_peer(d)):
                copy.wait_send()

        def end_query(k):
            for copy in query_copies(z - PLANES * (k + 1), z):
                copy.wait_send()

        def end_result(m):
            for copy in result_copies(z + PLANES * m, z):
                copy.wait_send()

        loop(1, NX, end_keys)
        loop(0, zp, end_query)
        loop(1, groups - zp, end_result)

    ends.append(end_attend)

    def stat_copy(n, d):
        return rcopy(stat.at[n], stats.at[n, d], ss.at[n, d], sr.at[n, d], sp, lax.rem(tp + d, ntp))

    def begin_tp(n, rows8):
        stat[n] = rows8
        loop(1, ntp, lambda d: stat_copy(n, d).start())
        ends.append(lambda: loop(1, ntp, lambda d: stat_copy(n, d).wait_send()))

    def finish_tp(n, rows8):
        loop(1, ntp, lambda d: stat_copy(n, d).wait_recv())
        total = rows8
        for d in range(1, ntp):
            total = total + stats[n, d]
        return total

    def halves_of(both):
        left, right = both[:, :128], both[:, 128:]
        return jnp.where(c == 0, left, right), jnp.where(c == 0, right, left)

    halves = ((0, 128), (128, 256))
    misc[...] = jnp.zeros((8, 128), f32)
    misc[0:2, :] = ids_ref[...].astype(f32)
    misc[2:4, :] = route_ref[...]
    facts = misc[...]
    id_cols = spread(facts, (0, 1), halves)
    route_cols = spread(facts, (2, 3), halves)
    lane128 = iota((128, 128), 1)
    lane_f = lane128.astype(f32)
    id_col = (id_cols[:, :128], id_cols[:, 128:])
    hot = [v == lane_f for v in id_col]
    tri = ones_where(iota((128, 128), 0) > lane128)
    earlier = dot(tri, ones_where(hot[0] | hot[1]))
    lane_all = iota((128, nsp * STRIDE), 1).astype(f32)
    choice = []
    for k in range(2):
        slot = jnp.sum(jnp.where(hot[k], earlier, 0.0), axis=1, keepdims=True)
        place = id_col[k][:, :1] * float(STRIDE) + slot
        choice.append(ones_where(place == lane_all))
    row_c, col_c = iota((nsp * CAP, nsp * STRIDE), 0), iota((nsp * CAP, nsp * STRIDE), 1)
    block_c = (row_c * (-(-(1 << 17) // CAP))) >> 17
    compact = ones_where(col_c == row_c + block_c * (STRIDE - CAP))

    own_squares = rowsums(attend * attend)
    begin_tp(0, own_squares)
    squares = finish_tp(0, own_squares)
    scale = spread(lax.rsqrt(squares / float(columns) + norm_eps), (0, 4), halves)
    normed_a = (attend[:, :128] * scale[:, :128] * ga_ref[...]).astype(bf16)
    normed_b = (attend[:, 128:] * scale[:, 128:] * gb_ref[...]).astype(bf16)
    loads[0].wait()
    loads[1].wait()

    def project(yy):
        cols = pl.ds(pl.multiple_of(yy * 256, 256), 256)
        return dot(normed_a, pa[:, cols]) + dot(normed_b, pb[:, cols])

    def mate1(d):
        return rcopy(p1s.at[d], p1v.at[d], p1ss.at[d], p1sr.at[d], sp, mate)

    def chip1(d):
        return rcopy(p1r.at[d], p1i.at[d], p1rs.at[d], p1rr.at[d], sp, lax.rem(y + d, ny) * 2 + c)

    def make1(d):
        own, other = halves_of(project(lax.rem(y + d, ny)))
        p1s[d] = other.astype(bf16)
        mate1(d).start()
        p1o[d] = own

    def pass1(d):
        mate1(d).wait_recv()
        p1r[d] = (p1o[d] + p1v[d].astype(f32)).astype(bf16)
        chip1(d).start()

    order = near_order(ny)[::-1]
    make1(order[0])
    for before, d in zip(order, order[1:] + [0]):
        make1(d)
        pass1(before)
    mate1(0).wait_recv()
    mixed = p1o[0] + p1v[0].astype(f32)
    for d in order[::-1]:
        chip1(d).wait_recv()
        mixed = mixed + p1i[d].astype(f32)
    ends.append(lambda: loop(0, ny, lambda d: mate1(d).wait_send()))
    ends.append(lambda: loop(1, ny, lambda d: chip1(d).wait_send()))
    first = depth_scale * res_ref[...].astype(f32) + mixed.astype(bf16).astype(f32)

    def begin_norm(n, total):
        sums = rowsums(jnp.concatenate([total, total * total], axis=1))
        begin_tp(n, sums)
        return sums

    def moments(n, sums):
        sums = finish_tp(n, sums)
        mean = sums[0:1, :] / float(columns)
        var = sums[4:5, :] / float(columns) - mean * mean
        return spread(jnp.where(row8 < 4, mean, lax.rsqrt(var + norm_eps)), (0, 4), halves)

    def normed(total, wide, gain, bias):
        return ((total - wide[:, :128]) * wide[:, 128:] * gain + bias).astype(bf16)

    own_sums = begin_norm(1, first)

    here = pl.ds(pl.multiple_of(sp * STRIDE, STRIDE), STRIDE)

    def sp_copy(src, dst, send, recv, d):
        peer = lax.rem(sp + d, nsp)
        rows = pl.ds(pl.multiple_of(peer * STRIDE, STRIDE), STRIDE)
        return rcopy(src.at[rows, :], dst.at[here, :], send.at[d], recv.at[d], peer, tp)

    def sp_await(src, dst, send, recv, d):
        peer = lax.rem(sp - d + nsp, nsp)
        rows = pl.ds(pl.multiple_of(peer * STRIDE, STRIDE), STRIDE)
        rcopy(src.at[rows, :], dst.at[rows, :], send.at[d], recv.at[d], peer, tp).wait_recv()

    def post(src, dst, send, recv, value):
        src[...] = value
        loop(1, nsp, lambda d: sp_copy(src, dst, send, recv, d).start())
        ends.append(lambda: loop(1, nsp, lambda d: sp_copy(src, dst, send, recv, d).wait_send()))
        dst[here, :] = src[here, :]

    def collect(src, dst, send, recv):
        loop(1, nsp, lambda d: sp_await(src, dst, send, recv, d))
        return dst[...]

    routes = choice[0] + choice[1]
    post(dsp, drv, ds_, dr_, dot_tl(routes, first.astype(bf16)).astype(bf16))
    wide = moments(1, own_sums)
    pieces = split(wide[:, :128], 3) + split(wide[:, 128:], 3)
    packed = jnp.zeros((128, 128), f32)
    for i, piece in enumerate(pieces):
        packed = jnp.where(lane128 == i, piece.astype(f32), packed)
    post(ssp, srv, ds2, dr2, dot_tl(routes, packed.astype(bf16)).astype(bf16))
    settled = normed(first, wide, gs_ref[...], bs_ref[...])
    tokens = dot(compact, collect(dsp, drv, ds_, dr_)).astype(bf16)

    half = ny // 2
    height = nsp * CAP // PIECES
    ways = (0, 1)

    def chip_at(steps):
        return lax.rem(y + steps + ny, ny)

    def last_hop(way, p):
        return half if (p < PIECES // 2) == (way == 0) else half - 1

    def block_of(way, hop, core):
        source = chip_at(-hop if way == 0 else hop)
        return source, pl.ds(pl.multiple_of(core * 128, 128), 128)

    def along(way, hop, p):
        source, side = block_of(way, hop, c)
        block = xg.at[source, pl.ds(p * height, height), side]
        target = chip_at(1 if way == 0 else -1) * 2 + c
        return rcopy(block, block, as_.at[way, hop, p], ar_.at[way, hop + 1, p], sp, target)

    def along_await(way, hop, p):
        source, side = block_of(way, hop, c)
        block = xg.at[source, pl.ds(p * height, height), side]
        target = chip_at(-1 if way == 0 else 1) * 2 + c
        rcopy(block, block, as_.at[way, hop, p], ar_.at[way, hop, p], sp, target).wait_recv()

    def across(way, hop, p):
        source, side = block_of(way, hop, c)
        block = xg.at[source, pl.ds(p * height, height), side]
        return rcopy(block, block, hs_.at[way, hop, p], hr_.at[way, hop, p], sp, mate)

    def across_await(way, hop, p):
        source, side = block_of(way, hop, 1 - c)
        block = xg.at[source, pl.ds(p * height, height), side]
        rcopy(block, block, hs_.at[way, hop, p], hr_.at[way, hop, p], sp, mate).wait_recv()

    def take(source, start):
        rows = pl.ds(pl.multiple_of(source * 256, 256), 256)
        block = xg[source].astype(f32)
        mean, factor = mr[:, :128], mr[:, 128:]
        sides = []
        for i in range(2):
            gain, bias = vecs[source * 2 + i, 0:1, :], vecs[source * 2 + i, 1:2, :]
            sides.append((block[:, i * 128 : i * 128 + 128] - mean) * factor * gain + bias)
        block = jnp.concatenate(sides, axis=1).astype(bf16)
        gate, up = dot(block, wg[rows, :]), dot(block, wu[rows, :])
        if start:
            acc_g[...] = gate
            acc_u[...] = up
        else:
            acc_g[...] += gate
            acc_u[...] += up

    xg[y, :, pl.ds(pl.multiple_of(c * 128, 128), 128)] = tokens
    sends = [(way, 0, p) for p in range(PIECES) for way in ways if last_hop(way, p) > 0]
    crossings = [(0, 0, p) for p in range(PIECES)]
    for key in sends:
        along(*key).start()
    for key in crossings:
        across(*key).start()
    loads[2].wait()
    loads[3].wait()
    loop(1, ntp, vec_await)
    row_m, col_m = iota((128, 256), 0), iota((128, 256), 1)
    unpack = ones_where(((row_m < 3) & (col_m < 128)) | ((row_m >= 3) & (row_m < 6) & (col_m >= 128)))
    numbers = dot(compact, collect(ssp, srv, ds2, dr2)).astype(bf16)
    mr[...] = dot(numbers, unpack)
    for p in range(PIECES):
        across_await(0, 0, p)
    take(y, True)
    for hop in range(1, half + 1):
        reached = [(way, hop, p) for p in range(PIECES) for way in ways if hop <= last_hop(way, p)]
        for key in reached:
            way, _, p = key
            along_await(*key)
            if hop < last_hop(way, p):
                along(*key).start()
                sends.append(key)
            across(*key).start()
            crossings.append(key)
        for key in reached:
            across_await(*key)
        take(chip_at(-hop), False)
        if hop < half:
            take(chip_at(hop), False)

    def end_gather():
        for key in sends:
            along(*key).wait_send()
        for key in crossings:
            across(*key).wait_send()

    ends.append(end_gather)

    gate = acc_g[...]
    hidden = (gate / (1.0 + jnp.exp(-gate)) * acc_u[...]).astype(bf16)
    loads[4].wait()

    def mate2(d):
        return rcopy(p2s.at[d], p2v.at[d], p2ss.at[d], p2sr.at[d], sp, mate)

    def make2(d):
        cols = pl.ds(pl.multiple_of(lax.rem(y + d, ny) * 256, 256), 256)
        own, other = halves_of(dot(hidden, wd[:, cols]))
        p2s[d] = other.astype(bf16)
        mate2(d).start()
        p2o[d] = own

    def term2(d, p):
        rows = slice(p * height, p * height + height)
        return p2o[d, rows, :] + p2v[d, rows, :].astype(f32)

    def pass2(way, step, p):
        rows = pl.ds(p * height, height)
        target = chip_at(1 if way == 0 else -1) * 2 + c
        return rcopy(
            rb_s.at[way, step, rows, :], rb_r.at[way, step, rows, :],
            rbs_.at[way, step, p], rbr_.at[way, step, p], sp, target,
        )

    passes = []

    def hand_on(step):
        left = half - step
        for p in range(PIECES):
            for way in ways:
                start = half - last_hop(way, p)
                if step < start:
                    continue
                rows = slice(p * height, p * height + height)
                value = term2(left if way == 0 else ny - left, p)
                if step > start:
                    pass2(way, step - 1, p).wait_recv()
                    value = value + rb_r[way, step - 1, rows, :].astype(f32)
                rb_s[way, step, rows, :] = value.astype(bf16)
                pass2(way, step, p).start()
                passes.append((way, step, p))

    make2(half)
    for step in range(half):
        left = half - step
        if left > 1:
            make2(left - 1)
            make2(ny - left + 1)
        else:
            make2(0)
        mate2(left).wait_recv()
        if left < half:
            mate2(ny - left).wait_recv()
        hand_on(step)
    mate2(0).wait_recv()
    outputs = []
    for p in range(PIECES):
        rows = slice(p * height, p * height + height)
        value = term2(0, p)
        for way in ways:
            if last_hop(way, p) > 0:
                pass2(way, half - 1, p).wait_recv()
                value = value + rb_r[way, half - 1, rows, :].astype(f32)
        outputs.append(value.astype(bf16))

    def end_sum():
        loop(0, ny, lambda d: mate2(d).wait_send())
        for key in passes:
            pass2(*key).wait_send()

    ends.append(end_sum)
    outputs = jnp.concatenate(outputs, axis=0)

    post(rts, rtv, ts_, tr_, dot_tl(compact, outputs).astype(bf16))
    returned = collect(rts, rtv, ts_, tr_)
    routed = route_cols[:, :128] * dot(choice[0], returned) + route_cols[:, 128:] * dot(choice[1], returned)
    second = depth_scale * settled.astype(f32) + routed
    last_sums = begin_norm(2, second)
    out_ref[...] = normed(second, moments(2, last_sums), gf_ref[...], bf_ref[...])
    for end in ends:
        end()


def body(
    nsp, ntp,
    residual_in, query_alpha, pairs_alpha, offset_alpha, gain_alpha,
    query_beta, pairs_beta, offset_beta, gain_beta, project_alpha, project_beta,
    gain_settle, bias_settle, expert_ids, route_weight,
    expert_gate, expert_up, expert_down, gain_final, bias_final,
):
    nz, ny = nsp // NX, ntp // 2
    vmem = pl.BlockSpec(memory_space=pltpu.VMEM)
    hbm = pl.BlockSpec(memory_space=pl.ANY)
    dma = pltpu.SemaphoreType.DMA
    V = pltpu.VMEM
    rows = nsp * CAP
    wide = nsp * STRIDE
    keys = PLANES * NX * 128
    half = ny // 2
    weights = (project_alpha, project_beta, expert_gate[0], expert_up[0], expert_down[0])
    vectors = [
        v.reshape(1, 128) for v in (gain_alpha, gain_beta, gain_settle, bias_settle, gain_final, bias_final)
    ]
    scratch = [V(w.shape, bf16) for w in weights] + [dma((5,)), V((8, 128), f32)]
    scratch += [
        V((keys, 128), bf16), V((keys, 128), bf16), V((keys, 256), bf16),
        V((8, 128), f32), V((8, keys), f32), V((nz, 128, 128), bf16), V((nz, 128, 128), bf16),
        V((nz, 128, 256), bf16), V((nz, 128, 256), bf16), V((nz, 8, 128), f32), V((nz, 8, 128), f32),
        dma((3, 2 * NX)), dma((3, 2 * NX)), dma((2, nz)), dma((2, nz)), dma((2, nz)), dma((2, nz)),
    ]
    scratch += [
        V((8, 128), f32), V((ntp, 8, 128), f32), dma((ntp,)), dma((ntp,)), V((rows, 256), f32),
        V((wide, 128), bf16), V((wide, 128), bf16), dma((nsp,)), dma((nsp,)),
    ]
    scratch += [V((3, 8, 128), f32), V((3, ntp, 8, 128), f32), dma((3, ntp)), dma((3, ntp))]
    scratch += [
        V((ny, 128, 128), bf16), V((ny, 128, 128), f32), V((ny, 128, 128), bf16),
        V((ny, 128, 128), bf16), V((ny, 128, 128), bf16), dma((ny,)), dma((ny,)), dma((ny,)), dma((ny,)),
    ]
    scratch += [V((wide, 128), bf16), V((wide, 128), bf16), dma((nsp,)), dma((nsp,))]
    hops = (2, half + 1, PIECES)
    scratch += [
        V((ny, rows, 256), bf16), dma(hops), dma(hops), dma(hops), dma(hops),
        V((rows, expert_gate.shape[2]), f32), V((rows, expert_gate.shape[2]), f32),
    ]
    scratch += [
        V((ny, rows, 128), bf16), V((ny, rows, 128), f32), V((ny, rows, 128), bf16), dma((ny,)), dma((ny,)),
        V((2, half, rows, 128), bf16), V((2, half, rows, 128), bf16), dma(hops), dma(hops),
    ]
    scratch += [V((wide, 128), bf16), V((wide, 128), bf16), dma((nsp,)), dma((nsp,))]
    return pl.pallas_call(
        functools.partial(layer_kernel, nsp, ntp),
        out_shape=jax.ShapeDtypeStruct((128, 128), bf16),
        in_specs=[vmem] * 15 + [hbm] * 5,
        out_specs=vmem,
        scratch_shapes=scratch,
        compiler_params=pltpu.CompilerParams(
            collective_id=0, has_side_effects=True, vmem_limit_bytes=62 * 1024 * 1024
        ),
        name="layer",
    )(
        query_alpha, query_beta, pairs_alpha.reshape(128, 128), pairs_beta.reshape(128, 256),
        offset_alpha.T, offset_beta.T, residual_in, *vectors, expert_ids.T, route_weight.T, *weights,
    )


def solution(mesh):
    in_specs = (
        P("sp", "tp"),
        P("sp", "tp"),
        P("sp", "tp", None),
        P("sp", "tp"),
        P("tp"),
        P("sp", "tp"),
        P("sp", "tp", None),
        P("sp", "tp"),
        P("tp"),
        P("tp", None),
        P("tp", None),
        P("tp"),
        P("tp"),
        P("sp", None),
        P("sp", None),
        P("sp", None, "tp"),
        P("sp", None, "tp"),
        P("sp", "tp", None),
        P("tp"),
        P("tp"),
    )
    step = functools.partial(body, mesh.shape["sp"], mesh.shape["tp"])
    return jax.shard_map(step, mesh=mesh, in_specs=in_specs, out_specs=P("sp", "tp"), check_vma=False)
```

```python
import functools
import jax
import jax.numpy as jnp
from jax import lax
from jax.experimental import pallas as pl
from jax.experimental.pallas import tpu as pltpu
from jax.sharding import PartitionSpec as P

depth_scale = 2.0**0.5
norm_eps = 1e-05
MESH = pl.DeviceIdType.MESH
NX = 4
CAP = 12
STRIDE = 16
PIECES = 4
PLANES = 2
bf16 = jnp.bfloat16
f32 = jnp.float32


def iota(shape, dim):
    return lax.broadcasted_iota(jnp.int32, shape, dim)


def ones_where(cond):
    return jnp.where(cond, 1.0, 0.0).astype(bf16)


def dot(a, b):
    return jnp.dot(a, b, preferred_element_type=f32)


def dot_tr(a, b):
    return lax.dot_general(a, b, (((1,), (1,)), ((), ())), preferred_element_type=f32)


def dot_tl(a, b):
    return lax.dot_general(a, b, (((0,), (0,)), ((), ())), preferred_element_type=f32)


def split(v, pieces):
    found = []
    for _ in range(pieces):
        part = v.astype(bf16)
        found.append(part)
        v = v - part.astype(f32)
    return found


def spread(rows8, low, high):
    parts = [p.astype(f32) for p in split(rows8, 3)] + [jnp.zeros_like(rows8)]
    stacked = jnp.concatenate(parts, axis=0).astype(bf16)
    row = iota((32, 256), 0)
    lane = iota((32, 256), 1)
    slot = row & 7
    pick = jnp.zeros((32, 256), jnp.bool_)
    for r, (first, last) in zip(low, high):
        pick = pick | ((slot == r) & (lane >= first) & (lane < last) & (row < 24))
    return dot_tl(stacked, ones_where(pick))


def rowsums(v):
    cat = jnp.concatenate(split(v, 3), axis=1)
    lane = iota((8, 768), 1) & 255
    row = iota((8, 768), 0)
    return dot_tr(ones_where((lane < 128) == (row < 4)), cat)


def rcopy(src, dst, send, recv, sp, tp):
    return pltpu.make_async_remote_copy(
        src_ref=src, dst_ref=dst, send_sem=send, recv_sem=recv, device_id=(sp, tp), device_id_type=MESH
    )


def loop(low, high, step):
    def run(i, carry):
        step(i)
        return carry

    lax.fori_loop(low, high, run, 0)


def near_order(n):
    return sorted(range(1, n), key=lambda d: (min(d, n - d), d))


def layer_kernel(
    nsp, ntp,
    qa_ref, qb_ref, ka_ref, kb_ref, oa_ref, ob_ref, res_ref, ga_ref, gb_ref, gs_ref, bs_ref, gf_ref, bf_ref,
    ids_ref, route_ref, pa_hbm, pb_hbm, wg_hbm, wu_hbm, wd_hbm, out_ref,
    held, hsem, pa, pb, wg, wu, wd, wsem, misc,
    kva, kvr, kvb, ofs, off, qba, qbb, ret, back, tot, tback,
    ks, kr, qs, qr, rs, rr,
    vec, vecs, vs_, vr_, mr, ssp, srv, ds2, dr2,
    stat, stats, ss, sr,
    p1s, p1o, p1v, p1r, p1i, p1ss, p1sr, p1rs, p1rr,
    dsp, drv, ds_, dr_,
    xg, as_, ar_, hs_, hr_, acc_g, acc_u,
    p2s, p2o, p2v, p2ss, p2sr, rb_s, rb_r, rbs_, rbr_,
    rts, rtv, ts_, tr_,
):
    sp, tp = lax.axis_index("sp"), lax.axis_index("tp")
    nz, ny = nsp // NX, ntp // 2
    z, x = lax.div(sp, NX), lax.rem(sp, NX)
    y, c = lax.div(tp, 2), lax.rem(tp, 2)
    mate = y * 2 + 1 - c
    columns = ntp * 128
    ends = []

    loads = [
        pltpu.make_async_copy(src, dst, wsem.at[i])
        for i, (src, dst) in enumerate(
            ((pa_hbm, pa), (pb_hbm, pb), (wg_hbm, wg), (wu_hbm, wu), (wd_hbm, wd))
        )
    ]
    given = (
        qa_ref, qb_ref, ka_ref, kb_ref, oa_ref, ob_ref, res_ref,
        ga_ref, gb_ref, gs_ref, bs_ref, gf_ref, bf_ref, ids_ref, route_ref,
    )
    fetches = [pltpu.make_async_copy(src, dst, hsem.at[i]) for i, (src, dst) in enumerate(zip(given, held))]
    for load in fetches:
        load.start()
    (
        qa_ref, qb_ref, ka_ref, kb_ref, oa_ref, ob_ref, res_ref,
        ga_ref, gb_ref, gs_ref, bs_ref, gf_ref, bf_ref, ids_ref, route_ref,
    ) = held

    barrier = pltpu.get_barrier_semaphore()

    def greet_sp(d):
        pl.semaphore_signal(barrier, 1, device_id=(lax.rem(sp + d, nsp), tp), device_id_type=MESH)

    def greet_tp(d):
        pl.semaphore_signal(barrier, 1, device_id=(sp, lax.rem(tp + d, ntp)), device_id_type=MESH)

    loop(1, nsp, greet_sp)
    loop(1, ntp, greet_tp)
    for load in fetches:
        load.wait()
    for load in loads:
        load.start()
    ofs[...] = jnp.zeros((8, 128), f32)
    ofs[0:2, :] = oa_ref[...]
    ofs[2:3, :] = ob_ref[...]
    vec[...] = jnp.zeros((8, 128), f32)
    vec[0:1, :] = gs_ref[...]
    vec[1:2, :] = bs_ref[...]
    pl.semaphore_wait(barrier, nsp - 1 + ntp - 1)

    groups = nz // PLANES
    zp, zb = lax.div(z, PLANES), lax.rem(z, PLANES)
    other_z = z + 1 - 2 * zb
    here_slot, there_slot = zb * NX, (1 - zb) * NX

    def key_copies(passed, k, slot, peer):
        rows = pl.ds(pl.multiple_of(slot * 128, 128), 128)
        sources = (kva.at[rows, :], kvb.at[rows, :], off.at[:, rows]) if passed else (ka_ref, kb_ref, ofs)
        targets = (kva.at[rows, :], kvb.at[rows, :], off.at[:, rows])
        return [
            rcopy(src, dst, ks.at[i, k], kr.at[i, k], peer, tp)
            for i, (src, dst) in enumerate(zip(sources, targets))
        ]

    def x_peer(d):
        return z * NX + lax.rem(x + d, NX)

    def cross_copies(slot):
        return key_copies(False, 0, slot + x, other_z * NX + x)

    def query_copies(dst_z, src_z):
        peer = dst_z * NX + x
        return (
            rcopy(qa_ref, qba.at[src_z], qs.at[0, dst_z], qr.at[0, src_z], peer, tp),
            rcopy(qb_ref, qbb.at[src_z], qs.at[1, dst_z], qr.at[1, src_z], peer, tp),
        )

    def result_copies(dst_z, src_z):
        peer = dst_z * NX + x
        return (
            rcopy(ret.at[dst_z], back.at[src_z], rs.at[0, dst_z], rr.at[0, src_z], peer, tp),
            rcopy(tot.at[dst_z], tback.at[src_z], rs.at[1, dst_z], rr.at[1, src_z], peer, tp),
        )

    for copy in cross_copies(here_slot):
        copy.start()

    def send_keys(d):
        for copy in key_copies(False, d, here_slot + x, x_peer(d)):
            copy.start()

    loop(1, NX, send_keys)

    def send_query(k):
        for copy in query_copies(z - PLANES * (k + 1), z):
            copy.start()

    loop(0, zp, send_query)

    def vec_copy(d):
        return rcopy(vec, vecs.at[tp], vs_.at[d], vr_.at[d], sp, lax.rem(tp + d, ntp))

    def vec_await(d):
        source = lax.rem(tp - d + ntp, ntp)
        rcopy(vec, vecs.at[source], vs_.at[d], vr_.at[d], sp, source).wait_recv()

    loop(1, ntp, lambda d: vec_copy(d).start())
    ends.append(lambda: loop(1, ntp, lambda d: vec_copy(d).wait_send()))
    vecs[tp] = vec[...]

    mine = pl.ds(pl.multiple_of((here_slot + x) * 128, 128), 128)
    kva[mine, :] = ka_ref[...]
    kvb[mine, :] = kb_ref[...]
    off[:, mine] = ofs[...]
    qba[z] = qa_ref[...]
    qbb[z] = qb_ref[...]

    for copy in cross_copies(there_slot):
        copy.wait_recv()

    def pass_keys(d):
        for copy in key_copies(True, NX + d, there_slot + x, x_peer(d)):
            copy.start()

    loop(1, NX, pass_keys)

    def await_keys(d):
        source = lax.rem(x - d + NX, NX)
        for copy in key_copies(False, d, here_slot + source, x_peer(d)):
            copy.wait_recv()
        for copy in key_copies(True, NX + d, there_slot + source, x_peer(d)):
            copy.wait_recv()

    loop(1, NX, await_keys)
    keys_a = kva[...]
    kvr[...] = pltpu.roll(keys_a.astype(f32), 64, 1).astype(bf16)

    lane = iota((128, 128), 1)
    gap = lane - iota((128, 128), 0)
    r256, c256 = iota((256, 256), 0) & 127, iota((256, 256), 1)
    later_matrix = ones_where((r256 > c256) | (c256 >= 128))
    first_lane = ones_where((iota((8, 384), 1) & 127) == 0)
    row8 = iota((8, 128), 0)

    def visit(m):
        zq = z + PLANES * m

        @pl.when(zq > z)
        def _():
            for copy in query_copies(z, zq):
                copy.wait_recv()

        qa, qb = qba[zq], qbb[zq]
        zero = jnp.zeros_like(qa)
        accs, totals = [], []
        for h in range(3):
            q = (jnp.where(lane < 64, qa, zero), jnp.where(lane >= 64, qa, zero), qb)[h]
            scale = (64.0**-0.5, 64.0**-0.5, 128.0**-0.5)[h]
            gone = jnp.zeros((128, 128), f32)
            weights = [None] * (PLANES * NX)
            for b in reversed(range(PLANES * NX)):
                rows = slice(b * 128, b * 128 + 128)
                keys = (kva[rows, :], kvr[rows, :], kvb[rows, :128])[h]
                scores = dot_tr(q, keys) * scale + off[h : h + 1, rows]
                valid = gap < ((zq - zp * PLANES) * NX + x - b) * 128
                soft = jnp.maximum(scores, 0.0) + jnp.log(1.0 + jnp.exp(-jnp.abs(scores)))
                cat = jnp.concatenate(split(jnp.where(valid, soft, 0.0), 2), axis=1)
                sums = dot(cat, later_matrix)
                power = (scores - soft) - (sums[:, :128] + gone)
                gone = gone + sums[:, 128:]
                weights[b] = jnp.where(valid, jnp.exp(power), 0.0).astype(bf16)
            values = (kvr[...], kva[...], kvb[:, 128:])[h]
            accs.append(dot(jnp.concatenate(weights, axis=1), values))
            totals.append(dot_tr(first_lane, jnp.concatenate(split(gone, 3), axis=1)))
        both = jnp.where(lane < 64, accs[0], accs[1])
        found = jnp.concatenate([both, accs[2]], axis=1).astype(bf16)
        sums8 = jnp.where(row8 == 0, totals[0], jnp.where(row8 == 1, totals[1], totals[2]))

        @pl.when(zq == z)
        def _():
            back[z] = found
            tback[z] = sums8

        @pl.when(zq > z)
        def _():
            ret[zq] = found
            tot[zq] = sums8
            for copy in result_copies(zq, z):
                copy.start()

    loop(0, groups - zp, visit)

    def gather(k, carry):
        acc, gone = carry
        zk = z - PLANES * k

        @pl.when(k > 0)
        def _():
            for copy in result_copies(z, zk):
                copy.wait_recv()

        wide = spread(jnp.exp(-gone), (0, 1, 2), ((0, 64), (64, 128), (128, 256)))
        return acc + wide * back[zk].astype(f32), gone + tback[zk]

    attend, _ = lax.fori_loop(
        0, zp + 1, gather, (jnp.zeros((128, 256), f32), jnp.zeros((8, 128), f32))
    )

    def end_attend():
        for copy in cross_copies(here_slot):
            copy.wait_send()

        def end_keys(d):
            for copy in key_copies(False, d, here_slot + x, x_peer(d)):
                copy.wait_send()
            for copy in key_copies(True, NX + d, there_slot + x, x_peer(d)):
                copy.wait_send()

        def end_query(k):
            for copy in query_copies(z - PLANES * (k + 1), z):
                copy.wait_send()

        def end_result(m):
            for copy in result_copies(z + PLANES * m, z):
                copy.wait_send()

        loop(1, NX, end_keys)
        loop(0, zp, end_query)
        loop(1, groups - zp, end_result)

    ends.append(end_attend)

    def stat_copy(n, d):
        return rcopy(stat.at[n], stats.at[n, d], ss.at[n, d], sr.at[n, d], sp, lax.rem(tp + d, ntp))

    def begin_tp(n, rows8):
        stat[n] = rows8
        loop(1, ntp, lambda d: stat_copy(n, d).start())
        ends.append(lambda: loop(1, ntp, lambda d: stat_copy(n, d).wait_send()))

    def finish_tp(n, rows8):
        loop(1, ntp, lambda d: stat_copy(n, d).wait_recv())
        total = rows8
        for d in range(1, ntp):
            total = total + stats[n, d]
        return total

    def halves_of(both):
        left, right = both[:, :128], both[:, 128:]
        return jnp.where(c == 0, left, right), jnp.where(c == 0, right, left)

    halves = ((0, 128), (128, 256))
    misc[...] = jnp.zeros((8, 128), f32)
    misc[0:2, :] = ids_ref[...].astype(f32)
    misc[2:4, :] = route_ref[...]
    facts = misc[...]
    id_cols = spread(facts, (0, 1), halves)
    route_cols = spread(facts, (2, 3), halves)
    lane128 = iota((128, 128), 1)
    lane_f = lane128.astype(f32)
    id_col = (id_cols[:, :128], id_cols[:, 128:])
    hot = [v == lane_f for v in id_col]
    tri = ones_where(iota((128, 128), 0) > lane128)
    earlier = dot(tri, ones_where(hot[0] | hot[1]))
    lane_all = iota((128, nsp * STRIDE), 1).astype(f32)
    choice = []
    for k in range(2):
        slot = jnp.sum(jnp.where(hot[k], earlier, 0.0), axis=1, keepdims=True)
        place = id_col[k][:, :1] * float(STRIDE) + slot
        choice.append(ones_where(place == lane_all))
    row_c, col_c = iota((nsp * CAP, nsp * STRIDE), 0), iota((nsp * CAP, nsp * STRIDE), 1)
    block_c = (row_c * (-(-(1 << 17) // CAP))) >> 17
    compact = ones_where(col_c == row_c + block_c * (STRIDE - CAP))

    own_squares = rowsums(attend * attend)
    begin_tp(0, own_squares)
    gained_a = (attend[:, :128] * ga_ref[...]).astype(bf16)
    gained_b = (attend[:, 128:] * gb_ref[...]).astype(bf16)
    loads[0].wait()
    loads[1].wait()

    def project(yy):
        cols = pl.ds(pl.multiple_of(yy * 256, 256), 256)
        return halves_of(dot(gained_a, pa[:, cols])), halves_of(dot(gained_b, pb[:, cols]))

    def mate1(d):
        return rcopy(p1s.at[d], p1v.at[d], p1ss.at[d], p1sr.at[d], sp, mate)

    def chip1(d):
        return rcopy(p1r.at[d], p1i.at[d], p1rs.at[d], p1rr.at[d], sp, lax.rem(y + d, ny) * 2 + c)

    def make1(d):
        (own_a, other_a), (own_b, other_b) = project(lax.rem(y + d, ny))
        p1s[d] = jnp.concatenate([other_a, other_b], axis=1).astype(bf16)
        mate1(d).start()
        p1o[d] = jnp.concatenate([own_a, own_b], axis=1)

    order = near_order(ny)[::-1]
    for d in order + [0]:
        make1(d)
    squares = finish_tp(0, own_squares)
    scale = spread(lax.rsqrt(squares / float(columns) + norm_eps), (0, 4), halves)

    def chip_sum(d):
        mate1(d).wait_recv()
        both = (p1o[d] + p1v[d].astype(f32)) * scale
        return both[:, :128] + both[:, 128:]

    for d in order:
        p1r[d] = chip_sum(d).astype(bf16)
        chip1(d).start()
    mixed = chip_sum(0)
    for d in order[::-1]:
        chip1(d).wait_recv()
        mixed = mixed + p1i[d].astype(f32)
    ends.append(lambda: loop(0, ny, lambda d: mate1(d).wait_send()))
    ends.append(lambda: loop(1, ny, lambda d: chip1(d).wait_send()))
    first = depth_scale * res_ref[...].astype(f32) + mixed.astype(bf16).astype(f32)

    def begin_norm(n, total):
        sums = rowsums(jnp.concatenate([total, total * total], axis=1))
        begin_tp(n, sums)
        return sums

    def moments(n, sums):
        sums = finish_tp(n, sums)
        mean = sums[0:1, :] / float(columns)
        var = sums[4:5, :] / float(columns) - mean * mean
        return spread(jnp.where(row8 < 4, mean, lax.rsqrt(var + norm_eps)), (0, 4), halves)

    def normed(total, wide, gain, bias):
        return ((total - wide[:, :128]) * wide[:, 128:] * gain + bias).astype(bf16)

    own_sums = begin_norm(1, first)

    here = pl.ds(pl.multiple_of(sp * STRIDE, STRIDE), STRIDE)

    def sp_copy(src, dst, send, recv, d):
        peer = lax.rem(sp + d, nsp)
        rows = pl.ds(pl.multiple_of(peer * STRIDE, STRIDE), STRIDE)
        return rcopy(src.at[rows, :], dst.at[here, :], send.at[d], recv.at[d], peer, tp)

    def sp_await(src, dst, send, recv, d):
        peer = lax.rem(sp - d + nsp, nsp)
        rows = pl.ds(pl.multiple_of(peer * STRIDE, STRIDE), STRIDE)
        rcopy(src.at[rows, :], dst.at[rows, :], send.at[d], recv.at[d], peer, tp).wait_recv()

    def post(src, dst, send, recv, value):
        src[...] = value
        loop(1, nsp, lambda d: sp_copy(src, dst, send, recv, d).start())
        ends.append(lambda: loop(1, nsp, lambda d: sp_copy(src, dst, send, recv, d).wait_send()))
        dst[here, :] = src[here, :]

    def collect(src, dst, send, recv):
        loop(1, nsp, lambda d: sp_await(src, dst, send, recv, d))
        return dst[...]

    routes = choice[0] + choice[1]
    post(dsp, drv, ds_, dr_, dot_tl(routes, first.astype(bf16)).astype(bf16))
    wide = moments(1, own_sums)
    pieces = split(wide[:, :128], 3) + split(wide[:, 128:], 3)
    packed = jnp.zeros((128, 128), f32)
    for i, piece in enumerate(pieces):
        packed = jnp.where(lane128 == i, piece.astype(f32), packed)
    post(ssp, srv, ds2, dr2, dot_tl(routes, packed.astype(bf16)).astype(bf16))
    settled = normed(first, wide, gs_ref[...], bs_ref[...])
    tokens = dot(compact, collect(dsp, drv, ds_, dr_)).astype(bf16)

    half = ny // 2
    height = nsp * CAP // PIECES
    ways = (0, 1)

    def chip_at(steps):
        return lax.rem(y + steps + ny, ny)

    def last_hop(way, p):
        return half if (p < PIECES // 2) == (way == 0) else half - 1

    def block_of(way, hop, core):
        source = chip_at(-hop if way == 0 else hop)
        return source, pl.ds(pl.multiple_of(core * 128, 128), 128)

    def along(way, hop, p):
        source, side = block_of(way, hop, c)
        block = xg.at[source, pl.ds(p * height, height), side]
        target = chip_at(1 if way == 0 else -1) * 2 + c
        return rcopy(block, block, as_.at[way, hop, p], ar_.at[way, hop + 1, p], sp, target)

    def along_await(way, hop, p):
        source, side = block_of(way, hop, c)
        block = xg.at[source, pl.ds(p * height, height), side]
        target = chip_at(-1 if way == 0 else 1) * 2 + c
        rcopy(block, block, as_.at[way, hop, p], ar_.at[way, hop, p], sp, target).wait_recv()

    def across(way, hop, p):
        source, side = block_of(way, hop, c)
        block = xg.at[source, pl.ds(p * height, height), side]
        return rcopy(block, block, hs_.at[way, hop, p], hr_.at[way, hop, p], sp, mate)

    def across_await(way, hop, p):
        source, side = block_of(way, hop, 1 - c)
        block = xg.at[source, pl.ds(p * height, height), side]
        rcopy(block, block, hs_.at[way, hop, p], hr_.at[way, hop, p], sp, mate).wait_recv()

    def take(source, start):
        rows = pl.ds(pl.multiple_of(source * 256, 256), 256)
        block = xg[source].astype(f32)
        mean, factor = mr[:, :128], mr[:, 128:]
        sides = []
        for i in range(2):
            gain, bias = vecs[source * 2 + i, 0:1, :], vecs[source * 2 + i, 1:2, :]
            sides.append((block[:, i * 128 : i * 128 + 128] - mean) * factor * gain + bias)
        block = jnp.concatenate(sides, axis=1).astype(bf16)
        gate, up = dot(block, wg[rows, :]), dot(block, wu[rows, :])
        if start:
            acc_g[...] = gate
            acc_u[...] = up
        else:
            acc_g[...] += gate
            acc_u[...] += up

    xg[y, :, pl.ds(pl.multiple_of(c * 128, 128), 128)] = tokens
    sends = [(way, 0, p) for p in range(PIECES) for way in ways if last_hop(way, p) > 0]
    crossings = [(0, 0, p) for p in range(PIECES)]
    for key in sends:
        along(*key).start()
    for key in crossings:
        across(*key).start()
    def advance(hop):
        reached = [(way, hop, p) for p in range(PIECES) for way in ways if hop <= last_hop(way, p)]
        for key in reached:
            way, _, p = key
            along_await(*key)
            if hop < last_hop(way, p):
                along(*key).start()
                sends.append(key)
            across(*key).start()
            crossings.append(key)
        return reached

    def consume(hop, reached):
        for key in reached:
            across_await(*key)
        take(chip_at(-hop), hop == 0)
        if 0 < hop < half:
            take(chip_at(hop), False)

    before = list(crossings)
    following = advance(1)
    loads[2].wait()
    loads[3].wait()
    loop(1, ntp, vec_await)
    row_m, col_m = iota((128, 256), 0), iota((128, 256), 1)
    unpack = ones_where(((row_m < 3) & (col_m < 128)) | ((row_m >= 3) & (row_m < 6) & (col_m >= 128)))
    numbers = dot(compact, collect(ssp, srv, ds2, dr2)).astype(bf16)
    mr[...] = dot(numbers, unpack)
    consume(0, before)
    for hop in range(1, half + 1):
        before = following
        if hop < half:
            following = advance(hop + 1)
        consume(hop, before)

    def end_gather():
        for key in sends:
            along(*key).wait_send()
        for key in crossings:
            across(*key).wait_send()

    ends.append(end_gather)

    gate = acc_g[...]
    hidden = (gate / (1.0 + jnp.exp(-gate)) * acc_u[...]).astype(bf16)
    loads[4].wait()

    def mate2(d):
        return rcopy(p2s.at[d], p2v.at[d], p2ss.at[d], p2sr.at[d], sp, mate)

    def make2(d):
        cols = pl.ds(pl.multiple_of(lax.rem(y + d, ny) * 256, 256), 256)
        own, other = halves_of(dot(hidden, wd[:, cols]))
        p2s[d] = other.astype(bf16)
        mate2(d).start()
        p2o[d] = own

    def term2(d, p):
        rows = slice(p * height, p * height + height)
        return p2o[d, rows, :] + p2v[d, rows, :].astype(f32)

    def pass2(way, step, p):
        rows = pl.ds(p * height, height)
        target = chip_at(1 if way == 0 else -1) * 2 + c
        return rcopy(
            rb_s.at[way, step, rows, :], rb_r.at[way, step, rows, :],
            rbs_.at[way, step, p], rbr_.at[way, step, p], sp, target,
        )

    passes = []

    def hand_on(step):
        left = half - step
        for p in range(PIECES):
            for way in ways:
                start = half - last_hop(way, p)
                if step < start:
                    continue
                rows = slice(p * height, p * height + height)
                value = term2(left if way == 0 else ny - left, p)
                if step > start:
                    pass2(way, step - 1, p).wait_recv()
                    value = value + rb_r[way, step - 1, rows, :].astype(f32)
                rb_s[way, step, rows, :] = value.astype(bf16)
                pass2(way, step, p).start()
                passes.append((way, step, p))

    make2(half)
    for step in range(half):
        left = half - step
        if left > 1:
            make2(left - 1)
            make2(ny - left + 1)
        else:
            make2(0)
        mate2(left).wait_recv()
        if left < half:
            mate2(ny - left).wait_recv()
        hand_on(step)
    mate2(0).wait_recv()
    outputs = []
    for p in range(PIECES):
        rows = slice(p * height, p * height + height)
        value = term2(0, p)
        for way in ways:
            if last_hop(way, p) > 0:
                pass2(way, half - 1, p).wait_recv()
                value = value + rb_r[way, half - 1, rows, :].astype(f32)
        outputs.append(value.astype(bf16))

    def end_sum():
        loop(0, ny, lambda d: mate2(d).wait_send())
        for key in passes:
            pass2(*key).wait_send()

    ends.append(end_sum)
    outputs = jnp.concatenate(outputs, axis=0)

    post(rts, rtv, ts_, tr_, dot_tl(compact, outputs).astype(bf16))
    returned = collect(rts, rtv, ts_, tr_)
    routed = route_cols[:, :128] * dot(choice[0], returned) + route_cols[:, 128:] * dot(choice[1], returned)
    second = depth_scale * settled.astype(f32) + routed
    last_sums = begin_norm(2, second)
    out_ref[...] = normed(second, moments(2, last_sums), gf_ref[...], bf_ref[...])
    for end in ends:
        end()


def body(
    nsp, ntp,
    residual_in, query_alpha, pairs_alpha, offset_alpha, gain_alpha,
    query_beta, pairs_beta, offset_beta, gain_beta, project_alpha, project_beta,
    gain_settle, bias_settle, expert_ids, route_weight,
    expert_gate, expert_up, expert_down, gain_final, bias_final,
):
    nz, ny = nsp // NX, ntp // 2
    vmem = pl.BlockSpec(memory_space=pltpu.VMEM)
    hbm = pl.BlockSpec(memory_space=pl.ANY)
    dma = pltpu.SemaphoreType.DMA
    V = pltpu.VMEM
    rows = nsp * CAP
    wide = nsp * STRIDE
    keys = PLANES * NX * 128
    half = ny // 2
    weights = (project_alpha, project_beta, expert_gate[0], expert_up[0], expert_down[0])
    vectors = [
        v.reshape(1, 128) for v in (gain_alpha, gain_beta, gain_settle, bias_settle, gain_final, bias_final)
    ]
    inputs = (
        query_alpha, query_beta, pairs_alpha.reshape(128, 128), pairs_beta.reshape(128, 256),
        offset_alpha.T, offset_beta.T, residual_in, *vectors, expert_ids.T, route_weight.T,
    )
    scratch = [tuple(V(a.shape, a.dtype) for a in inputs), dma((len(inputs),))]
    scratch += [V(w.shape, bf16) for w in weights] + [dma((5,)), V((8, 128), f32)]
    scratch += [
        V((keys, 128), bf16), V((keys, 128), bf16), V((keys, 256), bf16),
        V((8, 128), f32), V((8, keys), f32), V((nz, 128, 128), bf16), V((nz, 128, 128), bf16),
        V((nz, 128, 256), bf16), V((nz, 128, 256), bf16), V((nz, 8, 128), f32), V((nz, 8, 128), f32),
        dma((3, 2 * NX)), dma((3, 2 * NX)), dma((2, nz)), dma((2, nz)), dma((2, nz)), dma((2, nz)),
    ]
    scratch += [
        V((8, 128), f32), V((ntp, 8, 128), f32), dma((ntp,)), dma((ntp,)), V((rows, 256), f32),
        V((wide, 128), bf16), V((wide, 128), bf16), dma((nsp,)), dma((nsp,)),
    ]
    scratch += [V((3, 8, 128), f32), V((3, ntp, 8, 128), f32), dma((3, ntp)), dma((3, ntp))]
    scratch += [
        V((ny, 128, 256), bf16), V((ny, 128, 256), f32), V((ny, 128, 256), bf16),
        V((ny, 128, 128), bf16), V((ny, 128, 128), bf16), dma((ny,)), dma((ny,)), dma((ny,)), dma((ny,)),
    ]
    scratch += [V((wide, 128), bf16), V((wide, 128), bf16), dma((nsp,)), dma((nsp,))]
    hops = (2, half + 1, PIECES)
    scratch += [
        V((ny, rows, 256), bf16), dma(hops), dma(hops), dma(hops), dma(hops),
        V((rows, expert_gate.shape[2]), f32), V((rows, expert_gate.shape[2]), f32),
    ]
    scratch += [
        V((ny, rows, 128), bf16), V((ny, rows, 128), f32), V((ny, rows, 128), bf16), dma((ny,)), dma((ny,)),
        V((2, half, rows, 128), bf16), V((2, half, rows, 128), bf16), dma(hops), dma(hops),
    ]
    scratch += [V((wide, 128), bf16), V((wide, 128), bf16), dma((nsp,)), dma((nsp,))]
    return pl.pallas_call(
        functools.partial(layer_kernel, nsp, ntp),
        out_shape=jax.ShapeDtypeStruct((128, 128), bf16),
        in_specs=[hbm] * 20,
        out_specs=vmem,
        scratch_shapes=scratch,
        compiler_params=pltpu.CompilerParams(
            collective_id=0, has_side_effects=True, vmem_limit_bytes=62 * 1024 * 1024
        ),
        name="layer",
    )(*inputs, *weights)


def solution(mesh):
    in_specs = (
        P("sp", "tp"),
        P("sp", "tp"),
        P("sp", "tp", None),
        P("sp", "tp"),
        P("tp"),
        P("sp", "tp"),
        P("sp", "tp", None),
        P("sp", "tp"),
        P("tp"),
        P("tp", None),
        P("tp", None),
        P("tp"),
        P("tp"),
        P("sp", None),
        P("sp", None),
        P("sp", None, "tp"),
        P("sp", None, "tp"),
        P("sp", "tp", None),
        P("tp"),
        P("tp"),
    )
    step = functools.partial(body, mesh.shape["sp"], mesh.shape["tp"])
    return jax.shard_map(step, mesh=mesh, in_specs=in_specs, out_specs=P("sp", "tp"), check_vma=False)
```

```python
import functools
import jax
import jax.numpy as jnp
from jax import lax
from jax.experimental import pallas as pl
from jax.experimental.pallas import tpu as pltpu
from jax.sharding import PartitionSpec as P

depth_scale = 2.0**0.5
norm_eps = 1e-05
MESH = pl.DeviceIdType.MESH
NX = 4
CAP = 12
STRIDE = 16
PIECES = 4
PLANES = 2
bf16 = jnp.bfloat16
f32 = jnp.float32


def iota(shape, dim):
    return lax.broadcasted_iota(jnp.int32, shape, dim)


def ones_where(cond):
    return jnp.where(cond, 1.0, 0.0).astype(bf16)


def dot(a, b):
    return jnp.dot(a, b, preferred_element_type=f32)


def dot_tr(a, b):
    return lax.dot_general(a, b, (((1,), (1,)), ((), ())), preferred_element_type=f32)


def dot_tl(a, b):
    return lax.dot_general(a, b, (((0,), (0,)), ((), ())), preferred_element_type=f32)


def split(v, pieces):
    found = []
    for _ in range(pieces):
        part = v.astype(bf16)
        found.append(part)
        v = v - part.astype(f32)
    return found


def spread(rows8, low, high):
    parts = [p.astype(f32) for p in split(rows8, 3)] + [jnp.zeros_like(rows8)]
    stacked = jnp.concatenate(parts, axis=0).astype(bf16)
    row = iota((32, 256), 0)
    lane = iota((32, 256), 1)
    slot = row & 7
    pick = jnp.zeros((32, 256), jnp.bool_)
    for r, (first, last) in zip(low, high):
        pick = pick | ((slot == r) & (lane >= first) & (lane < last) & (row < 24))
    return dot_tl(stacked, ones_where(pick))


def rowsums(v):
    cat = jnp.concatenate(split(v, 3), axis=1)
    lane = iota((8, 768), 1) & 255
    row = iota((8, 768), 0)
    return dot_tr(ones_where((lane < 128) == (row < 4)), cat)


def rcopy(src, dst, send, recv, sp, tp):
    return pltpu.make_async_remote_copy(
        src_ref=src, dst_ref=dst, send_sem=send, recv_sem=recv, device_id=(sp, tp), device_id_type=MESH
    )


def loop(low, high, step):
    def run(i, carry):
        step(i)
        return carry

    lax.fori_loop(low, high, run, 0)


def near_order(n):
    return sorted(range(1, n), key=lambda d: (min(d, n - d), d))


def layer_kernel(
    nsp, ntp,
    qa_ref, qb_ref, ka_ref, kb_ref, oa_ref, ob_ref, res_ref, ga_ref, gb_ref, gs_ref, bs_ref, gf_ref, bf_ref,
    ids_ref, route_ref, pa_hbm, pb_hbm, wg_hbm, wu_hbm, wd_hbm, out_ref,
    held, hsem, pa, pb, wg, wu, wd, wsem, misc,
    kva, kvr, kvb, ofs, off, qba, qbb, ret, back, tot, tback,
    ks, kr, qs, qr, rs, rr,
    vec, vecs, vs_, vr_, mr, ssp, srv, ds2, dr2,
    stat, stats, ss, sr,
    p1s, p1o, p1v, p1r, p1i, p1ss, p1sr, p1rs, p1rr,
    dsp, drv, ds_, dr_,
    xg, as_, ar_, hs_, hr_, acc_g, acc_u,
    p2s, p2o, p2v, p2ss, p2sr, rb_s, rb_r, rbs_, rbr_,
    rts, rtv, ts_, tr_,
):
    sp, tp = lax.axis_index("sp"), lax.axis_index("tp")
    nz, ny = nsp // NX, ntp // 2
    z, x = lax.div(sp, NX), lax.rem(sp, NX)
    y, c = lax.div(tp, 2), lax.rem(tp, 2)
    mate = y * 2 + 1 - c
    columns = ntp * 128
    ends = []

    loads = [
        pltpu.make_async_copy(src, dst, wsem.at[i])
        for i, (src, dst) in enumerate(
            ((pa_hbm, pa), (pb_hbm, pb), (wg_hbm, wg), (wu_hbm, wu), (wd_hbm, wd))
        )
    ]
    given = (
        qa_ref, qb_ref, ka_ref, kb_ref, oa_ref, ob_ref, res_ref,
        ga_ref, gb_ref, gs_ref, bs_ref, gf_ref, bf_ref, ids_ref, route_ref,
    )
    fetches = [pltpu.make_async_copy(src, dst, hsem.at[i]) for i, (src, dst) in enumerate(zip(given, held))]
    for load in fetches:
        load.start()
    (
        qa_ref, qb_ref, ka_ref, kb_ref, oa_ref, ob_ref, res_ref,
        ga_ref, gb_ref, gs_ref, bs_ref, gf_ref, bf_ref, ids_ref, route_ref,
    ) = held

    barrier = pltpu.get_barrier_semaphore()

    def greet_sp(d):
        pl.semaphore_signal(barrier, 1, device_id=(lax.rem(sp + d, nsp), tp), device_id_type=MESH)

    def greet_tp(d):
        pl.semaphore_signal(barrier, 1, device_id=(sp, lax.rem(tp + d, ntp)), device_id_type=MESH)

    loop(1, nsp, greet_sp)
    loop(1, ntp, greet_tp)
    for load in fetches:
        load.wait()
    for load in loads:
        load.start()
    ofs[...] = jnp.zeros((8, 128), f32)
    ofs[0:2, :] = oa_ref[...]
    ofs[2:3, :] = ob_ref[...]
    vec[...] = jnp.zeros((8, 128), f32)
    vec[0:1, :] = gs_ref[...]
    vec[1:2, :] = bs_ref[...]
    pl.semaphore_wait(barrier, nsp - 1 + ntp - 1)

    groups = nz // PLANES
    zp, zb = lax.div(z, PLANES), lax.rem(z, PLANES)
    other_z = z + 1 - 2 * zb
    here_slot, there_slot = zb * NX, (1 - zb) * NX

    def key_copies(passed, k, slot, peer):
        rows = pl.ds(pl.multiple_of(slot * 128, 128), 128)
        sources = (kva.at[rows, :], kvb.at[rows, :], off.at[:, rows]) if passed else (ka_ref, kb_ref, ofs)
        targets = (kva.at[rows, :], kvb.at[rows, :], off.at[:, rows])
        return [
            rcopy(src, dst, ks.at[i, k], kr.at[i, k], peer, tp)
            for i, (src, dst) in enumerate(zip(sources, targets))
        ]

    def x_peer(d):
        return z * NX + lax.rem(x + d, NX)

    def cross_copies(slot):
        return key_copies(False, 0, slot + x, other_z * NX + x)

    def query_copies(dst_z, src_z):
        peer = dst_z * NX + x
        return (
            rcopy(qa_ref, qba.at[src_z], qs.at[0, dst_z], qr.at[0, src_z], peer, tp),
            rcopy(qb_ref, qbb.at[src_z], qs.at[1, dst_z], qr.at[1, src_z], peer, tp),
        )

    def result_copies(dst_z, src_z):
        peer = dst_z * NX + x
        return (
            rcopy(ret.at[dst_z], back.at[src_z], rs.at[0, dst_z], rr.at[0, src_z], peer, tp),
            rcopy(tot.at[dst_z], tback.at[src_z], rs.at[1, dst_z], rr.at[1, src_z], peer, tp),
        )

    for copy in cross_copies(here_slot):
        copy.start()

    def send_keys(d):
        for copy in key_copies(False, d, here_slot + x, x_peer(d)):
            copy.start()

    loop(1, NX, send_keys)

    def send_query(k):
        for copy in query_copies(z - PLANES * (k + 1), z):
            copy.start()

    loop(0, zp, send_query)

    def vec_copy(d):
        return rcopy(vec, vecs.at[tp], vs_.at[d], vr_.at[d], sp, lax.rem(tp + d, ntp))

    def vec_await(d):
        source = lax.rem(tp - d + ntp, ntp)
        rcopy(vec, vecs.at[source], vs_.at[d], vr_.at[d], sp, source).wait_recv()

    loop(1, ntp, lambda d: vec_copy(d).start())
    ends.append(lambda: loop(1, ntp, lambda d: vec_copy(d).wait_send()))
    vecs[tp] = vec[...]

    mine = pl.ds(pl.multiple_of((here_slot + x) * 128, 128), 128)
    kva[mine, :] = ka_ref[...]
    kvb[mine, :] = kb_ref[...]
    off[:, mine] = ofs[...]
    qba[z] = qa_ref[...]
    qbb[z] = qb_ref[...]

    for copy in cross_copies(there_slot):
        copy.wait_recv()

    def pass_keys(d):
        for copy in key_copies(True, NX + d, there_slot + x, x_peer(d)):
            copy.start()

    loop(1, NX, pass_keys)

    def await_keys(d):
        source = lax.rem(x - d + NX, NX)
        for copy in key_copies(False, d, here_slot + source, x_peer(d)):
            copy.wait_recv()
        for copy in key_copies(True, NX + d, there_slot + source, x_peer(d)):
            copy.wait_recv()

    loop(1, NX, await_keys)
    keys_a = kva[...]
    kvr[...] = pltpu.roll(keys_a.astype(f32), 64, 1).astype(bf16)

    lane = iota((128, 128), 1)
    gap = lane - iota((128, 128), 0)
    r256, c256 = iota((256, 256), 0) & 127, iota((256, 256), 1)
    later_matrix = ones_where((r256 > c256) | (c256 >= 128))
    first_lane = ones_where((iota((8, 384), 1) & 127) == 0)
    row8 = iota((8, 128), 0)

    def visit(m, own):
        zq = z + PLANES * m
        if not own:
            for copy in query_copies(z, zq):
                copy.wait_recv()

        qa, qb = (qba[zq].astype(f32) * 64.0**-0.5).astype(bf16), qbb[zq]
        zero = jnp.zeros_like(qa)
        accs, totals = [], []
        for h in range(3):
            q = (jnp.where(lane < 64, qa, zero), jnp.where(lane >= 64, qa, zero), qb)[h]
            gone = jnp.zeros((128, 128), f32)
            weights = [None] * (PLANES * NX)
            for b in reversed(range(PLANES * NX)):
                rows = slice(b * 128, b * 128 + 128)
                keys = (kva[rows, :], kvr[rows, :], kvb[rows, :128])[h]
                scores = dot_tr(q, keys)
                scores = (scores * 128.0**-0.5 if h == 2 else scores) + off[h : h + 1, rows]
                valid = gap < ((zq - zp * PLANES) * NX + x - b) * 128
                soft = jnp.maximum(scores, 0.0) + jnp.log(1.0 + jnp.exp(-jnp.abs(scores)))
                cat = jnp.concatenate(split(jnp.where(valid, soft, 0.0) if own else soft, 2), axis=1)
                sums = dot(cat, later_matrix)
                power = (scores - soft) - (sums[:, :128] + gone)
                gone = gone + sums[:, 128:]
                weight = jnp.exp(power)
                weights[b] = (jnp.where(valid, weight, 0.0) if own else weight).astype(bf16)
            values = (kvr[...], kva[...], kvb[:, 128:])[h]
            accs.append(dot(jnp.concatenate(weights, axis=1), values))
            totals.append(dot_tr(first_lane, jnp.concatenate(split(gone, 3), axis=1)))
        both = jnp.where(lane < 64, accs[0], accs[1])
        found = jnp.concatenate([both, accs[2]], axis=1).astype(bf16)
        sums8 = jnp.where(row8 == 0, totals[0], jnp.where(row8 == 1, totals[1], totals[2]))

        if own:
            back[z] = found
            tback[z] = sums8
        else:
            ret[zq] = found
            tot[zq] = sums8
            for copy in result_copies(zq, z):
                copy.start()

    visit(0, True)
    loop(1, groups - zp, lambda m: visit(m, False))

    def gather(k, carry):
        acc, gone = carry
        zk = z - PLANES * k

        @pl.when(k > 0)
        def _():
            for copy in result_copies(z, zk):
                copy.wait_recv()

        wide = spread(jnp.exp(-gone), (0, 1, 2), ((0, 64), (64, 128), (128, 256)))
        return acc + wide * back[zk].astype(f32), gone + tback[zk]

    attend, _ = lax.fori_loop(
        0, zp + 1, gather, (jnp.zeros((128, 256), f32), jnp.zeros((8, 128), f32))
    )

    def end_attend():
        for copy in cross_copies(here_slot):
            copy.wait_send()

        def end_keys(d):
            for copy in key_copies(False, d, here_slot + x, x_peer(d)):
                copy.wait_send()
            for copy in key_copies(True, NX + d, there_slot + x, x_peer(d)):
                copy.wait_send()

        def end_query(k):
            for copy in query_copies(z - PLANES * (k + 1), z):
                copy.wait_send()

        def end_result(m):
            for copy in result_copies(z + PLANES * m, z):
                copy.wait_send()

        loop(1, NX, end_keys)
        loop(0, zp, end_query)
        loop(1, groups - zp, end_result)

    ends.append(end_attend)

    def stat_copy(n, d):
        return rcopy(stat.at[n], stats.at[n, d], ss.at[n, d], sr.at[n, d], sp, lax.rem(tp + d, ntp))

    def begin_tp(n, rows8):
        stat[n] = rows8
        loop(1, ntp, lambda d: stat_copy(n, d).start())
        ends.append(lambda: loop(1, ntp, lambda d: stat_copy(n, d).wait_send()))

    def finish_tp(n, rows8):
        loop(1, ntp, lambda d: stat_copy(n, d).wait_recv())
        total = rows8
        for d in range(1, ntp):
            total = total + stats[n, d]
        return total

    def halves_of(both):
        left, right = both[:, :128], both[:, 128:]
        return jnp.where(c == 0, left, right), jnp.where(c == 0, right, left)

    halves = ((0, 128), (128, 256))
    misc[...] = jnp.zeros((8, 128), f32)
    misc[0:2, :] = ids_ref[...].astype(f32)
    misc[2:4, :] = route_ref[...]
    facts = misc[...]
    id_cols = spread(facts, (0, 1), halves)
    route_cols = spread(facts, (2, 3), halves)
    lane128 = iota((128, 128), 1)
    lane_f = lane128.astype(f32)
    id_col = (id_cols[:, :128], id_cols[:, 128:])
    hot = [v == lane_f for v in id_col]
    tri = ones_where(iota((128, 128), 0) > lane128)
    earlier = dot(tri, ones_where(hot[0] | hot[1]))
    lane_all = iota((128, nsp * STRIDE), 1).astype(f32)
    choice = []
    for k in range(2):
        slot = jnp.sum(jnp.where(hot[k], earlier, 0.0), axis=1, keepdims=True)
        place = id_col[k][:, :1] * float(STRIDE) + slot
        choice.append(ones_where(place == lane_all))
    row_c, col_c = iota((nsp * CAP, nsp * STRIDE), 0), iota((nsp * CAP, nsp * STRIDE), 1)
    block_c = (row_c * (-(-(1 << 17) // CAP))) >> 17
    compact = ones_where(col_c == row_c + block_c * (STRIDE - CAP))

    own_squares = rowsums(attend * attend)
    begin_tp(0, own_squares)
    gained_a = (attend[:, :128] * ga_ref[...]).astype(bf16)
    gained_b = (attend[:, 128:] * gb_ref[...]).astype(bf16)
    loads[0].wait()
    loads[1].wait()

    def project(yy):
        cols = pl.ds(pl.multiple_of(yy * 256, 256), 256)
        return halves_of(dot(gained_a, pa[:, cols])), halves_of(dot(gained_b, pb[:, cols]))

    def mate1(d):
        return rcopy(p1s.at[d], p1v.at[d], p1ss.at[d], p1sr.at[d], sp, mate)

    def chip1(d):
        return rcopy(p1r.at[d], p1i.at[d], p1rs.at[d], p1rr.at[d], sp, lax.rem(y + d, ny) * 2 + c)

    def make1(d):
        (own_a, other_a), (own_b, other_b) = project(lax.rem(y + d, ny))
        p1s[d] = jnp.concatenate([other_a, other_b], axis=1).astype(bf16)
        mate1(d).start()
        p1o[d] = jnp.concatenate([own_a, own_b], axis=1)

    order = near_order(ny)[::-1]
    for d in order + [0]:
        make1(d)
    squares = finish_tp(0, own_squares)
    scale = spread(lax.rsqrt(squares / float(columns) + norm_eps), (0, 4), halves)

    def chip_sum(d):
        mate1(d).wait_recv()
        both = (p1o[d] + p1v[d].astype(f32)) * scale
        return both[:, :128] + both[:, 128:]

    for d in order:
        p1r[d] = chip_sum(d).astype(bf16)
        chip1(d).start()
    mixed = chip_sum(0)
    for d in order[::-1]:
        chip1(d).wait_recv()
        mixed = mixed + p1i[d].astype(f32)
    ends.append(lambda: loop(0, ny, lambda d: mate1(d).wait_send()))
    ends.append(lambda: loop(1, ny, lambda d: chip1(d).wait_send()))
    first = depth_scale * res_ref[...].astype(f32) + mixed.astype(bf16).astype(f32)

    def begin_norm(n, total):
        sums = rowsums(jnp.concatenate([total, total * total], axis=1))
        begin_tp(n, sums)
        return sums

    def moments(n, sums):
        sums = finish_tp(n, sums)
        mean = sums[0:1, :] / float(columns)
        var = sums[4:5, :] / float(columns) - mean * mean
        return spread(jnp.where(row8 < 4, mean, lax.rsqrt(var + norm_eps)), (0, 4), halves)

    def normed(total, wide, gain, bias):
        return ((total - wide[:, :128]) * wide[:, 128:] * gain + bias).astype(bf16)

    own_sums = begin_norm(1, first)

    here = pl.ds(pl.multiple_of(sp * STRIDE, STRIDE), STRIDE)

    def sp_copy(src, dst, send, recv, d):
        peer = lax.rem(sp + d, nsp)
        rows = pl.ds(pl.multiple_of(peer * STRIDE, STRIDE), STRIDE)
        return rcopy(src.at[rows, :], dst.at[here, :], send.at[d], recv.at[d], peer, tp)

    def sp_await(src, dst, send, recv, d):
        peer = lax.rem(sp - d + nsp, nsp)
        rows = pl.ds(pl.multiple_of(peer * STRIDE, STRIDE), STRIDE)
        rcopy(src.at[rows, :], dst.at[rows, :], send.at[d], recv.at[d], peer, tp).wait_recv()

    def post(src, dst, send, recv, value):
        src[...] = value
        loop(1, nsp, lambda d: sp_copy(src, dst, send, recv, d).start())
        ends.append(lambda: loop(1, nsp, lambda d: sp_copy(src, dst, send, recv, d).wait_send()))
        dst[here, :] = src[here, :]

    def collect(src, dst, send, recv):
        loop(1, nsp, lambda d: sp_await(src, dst, send, recv, d))
        return dst[...]

    routes = choice[0] + choice[1]
    post(dsp, drv, ds_, dr_, dot_tl(routes, first.astype(bf16)).astype(bf16))
    wide = moments(1, own_sums)
    pieces = split(wide[:, :128], 3) + split(wide[:, 128:], 3)
    packed = jnp.zeros((128, 128), f32)
    for i, piece in enumerate(pieces):
        packed = jnp.where(lane128 == i, piece.astype(f32), packed)
    post(ssp, srv, ds2, dr2, dot_tl(routes, packed.astype(bf16)).astype(bf16))
    settled = normed(first, wide, gs_ref[...], bs_ref[...])
    tokens = dot(compact, collect(dsp, drv, ds_, dr_)).astype(bf16)

    half = ny // 2
    height = nsp * CAP // PIECES
    ways = (0, 1)

    def chip_at(steps):
        return lax.rem(y + steps + ny, ny)

    def last_hop(way, p):
        return half if (p < PIECES // 2) == (way == 0) else half - 1

    def block_of(way, hop, core):
        source = chip_at(-hop if way == 0 else hop)
        return source, pl.ds(pl.multiple_of(core * 128, 128), 128)

    def along(way, hop, p):
        source, side = block_of(way, hop, c)
        block = xg.at[source, pl.ds(p * height, height), side]
        target = chip_at(1 if way == 0 else -1) * 2 + c
        return rcopy(block, block, as_.at[way, hop, p], ar_.at[way, hop + 1, p], sp, target)

    def along_await(way, hop, p):
        source, side = block_of(way, hop, c)
        block = xg.at[source, pl.ds(p * height, height), side]
        target = chip_at(-1 if way == 0 else 1) * 2 + c
        rcopy(block, block, as_.at[way, hop, p], ar_.at[way, hop, p], sp, target).wait_recv()

    def across(way, hop, p):
        source, side = block_of(way, hop, c)
        block = xg.at[source, pl.ds(p * height, height), side]
        return rcopy(block, block, hs_.at[way, hop, p], hr_.at[way, hop, p], sp, mate)

    def across_await(way, hop, p):
        source, side = block_of(way, hop, 1 - c)
        block = xg.at[source, pl.ds(p * height, height), side]
        rcopy(block, block, hs_.at[way, hop, p], hr_.at[way, hop, p], sp, mate).wait_recv()

    def take(source, start):
        rows = pl.ds(pl.multiple_of(source * 256, 256), 256)
        block = xg[source].astype(f32)
        mean, factor = mr[:, :128], mr[:, 128:]
        sides = []
        for i in range(2):
            gain, bias = vecs[source * 2 + i, 0:1, :], vecs[source * 2 + i, 1:2, :]
            sides.append((block[:, i * 128 : i * 128 + 128] - mean) * factor * gain + bias)
        block = jnp.concatenate(sides, axis=1).astype(bf16)
        gate, up = dot(block, wg[rows, :]), dot(block, wu[rows, :])
        if start:
            acc_g[...] = gate
            acc_u[...] = up
        else:
            acc_g[...] += gate
            acc_u[...] += up

    xg[y, :, pl.ds(pl.multiple_of(c * 128, 128), 128)] = tokens
    sends = [(way, 0, p) for p in range(PIECES) for way in ways if last_hop(way, p) > 0]
    crossings = [(0, 0, p) for p in range(PIECES)]
    for key in sends:
        along(*key).start()
    for key in crossings:
        across(*key).start()
    def advance(hop):
        reached = [(way, hop, p) for p in range(PIECES) for way in ways if hop <= last_hop(way, p)]
        for key in reached:
            way, _, p = key
            along_await(*key)
            if hop < last_hop(way, p):
                along(*key).start()
                sends.append(key)
            across(*key).start()
            crossings.append(key)
        return reached

    def consume(hop, reached):
        for key in reached:
            across_await(*key)
        take(chip_at(-hop), hop == 0)
        if 0 < hop < half:
            take(chip_at(hop), False)

    before = list(crossings)
    following = advance(1)
    loads[2].wait()
    loads[3].wait()
    loop(1, ntp, vec_await)
    row_m, col_m = iota((128, 256), 0), iota((128, 256), 1)
    unpack = ones_where(((row_m < 3) & (col_m < 128)) | ((row_m >= 3) & (row_m < 6) & (col_m >= 128)))
    numbers = dot(compact, collect(ssp, srv, ds2, dr2)).astype(bf16)
    mr[...] = dot(numbers, unpack)
    consume(0, before)
    for hop in range(1, half + 1):
        before = following
        if hop < half:
            following = advance(hop + 1)
        consume(hop, before)

    def end_gather():
        for key in sends:
            along(*key).wait_send()
        for key in crossings:
            across(*key).wait_send()

    ends.append(end_gather)

    gate = acc_g[...]
    hidden = (gate / (1.0 + jnp.exp(-gate)) * acc_u[...]).astype(bf16)
    loads[4].wait()

    def mate2(d):
        return rcopy(p2s.at[d], p2v.at[d], p2ss.at[d], p2sr.at[d], sp, mate)

    def make2(d):
        cols = pl.ds(pl.multiple_of(lax.rem(y + d, ny) * 256, 256), 256)
        own, other = halves_of(dot(hidden, wd[:, cols]))
        p2s[d] = other.astype(bf16)
        mate2(d).start()
        p2o[d] = own

    def term2(d, p):
        rows = slice(p * height, p * height + height)
        return p2o[d, rows, :] + p2v[d, rows, :].astype(f32)

    def pass2(way, step, p):
        rows = pl.ds(p * height, height)
        target = chip_at(1 if way == 0 else -1) * 2 + c
        return rcopy(
            rb_s.at[way, step, rows, :], rb_r.at[way, step, rows, :],
            rbs_.at[way, step, p], rbr_.at[way, step, p], sp, target,
        )

    passes = []

    def hand_on(step):
        left = half - step
        for p in range(PIECES):
            for way in ways:
                start = half - last_hop(way, p)
                if step < start:
                    continue
                rows = slice(p * height, p * height + height)
                value = term2(left if way == 0 else ny - left, p)
                if step > start:
                    pass2(way, step - 1, p).wait_recv()
                    value = value + rb_r[way, step - 1, rows, :].astype(f32)
                rb_s[way, step, rows, :] = value.astype(bf16)
                pass2(way, step, p).start()
                passes.append((way, step, p))

    make2(half)
    for step in range(half):
        left = half - step
        if left > 1:
            make2(left - 1)
            make2(ny - left + 1)
        else:
            make2(0)
        mate2(left).wait_recv()
        if left < half:
            mate2(ny - left).wait_recv()
        hand_on(step)
    mate2(0).wait_recv()
    outputs = []
    for p in range(PIECES):
        rows = slice(p * height, p * height + height)
        value = term2(0, p)
        for way in ways:
            if last_hop(way, p) > 0:
                pass2(way, half - 1, p).wait_recv()
                value = value + rb_r[way, half - 1, rows, :].astype(f32)
        outputs.append(value.astype(bf16))

    def end_sum():
        loop(0, ny, lambda d: mate2(d).wait_send())
        for key in passes:
            pass2(*key).wait_send()

    ends.append(end_sum)
    outputs = jnp.concatenate(outputs, axis=0)

    post(rts, rtv, ts_, tr_, dot_tl(compact, outputs).astype(bf16))
    returned = collect(rts, rtv, ts_, tr_)
    routed = route_cols[:, :128] * dot(choice[0], returned) + route_cols[:, 128:] * dot(choice[1], returned)
    second = depth_scale * settled.astype(f32) + routed
    last_sums = begin_norm(2, second)
    for end in ends[:-1]:
        end()
    out_ref[...] = normed(second, moments(2, last_sums), gf_ref[...], bf_ref[...])
    ends[-1]()


def body(
    nsp, ntp,
    residual_in, query_alpha, pairs_alpha, offset_alpha, gain_alpha,
    query_beta, pairs_beta, offset_beta, gain_beta, project_alpha, project_beta,
    gain_settle, bias_settle, expert_ids, route_weight,
    expert_gate, expert_up, expert_down, gain_final, bias_final,
):
    nz, ny = nsp // NX, ntp // 2
    vmem = pl.BlockSpec(memory_space=pltpu.VMEM)
    hbm = pl.BlockSpec(memory_space=pl.ANY)
    dma = pltpu.SemaphoreType.DMA
    V = pltpu.VMEM
    rows = nsp * CAP
    wide = nsp * STRIDE
    keys = PLANES * NX * 128
    half = ny // 2
    weights = (project_alpha, project_beta, expert_gate[0], expert_up[0], expert_down[0])
    vectors = [
        v.reshape(1, 128) for v in (gain_alpha, gain_beta, gain_settle, bias_settle, gain_final, bias_final)
    ]
    inputs = (
        query_alpha, query_beta, pairs_alpha.reshape(128, 128), pairs_beta.reshape(128, 256),
        offset_alpha.T, offset_beta.T, residual_in, *vectors, expert_ids.T, route_weight.T,
    )
    scratch = [tuple(V(a.shape, a.dtype) for a in inputs), dma((len(inputs),))]
    scratch += [V(w.shape, bf16) for w in weights] + [dma((5,)), V((8, 128), f32)]
    scratch += [
        V((keys, 128), bf16), V((keys, 128), bf16), V((keys, 256), bf16),
        V((8, 128), f32), V((8, keys), f32), V((nz, 128, 128), bf16), V((nz, 128, 128), bf16),
        V((nz, 128, 256), bf16), V((nz, 128, 256), bf16), V((nz, 8, 128), f32), V((nz, 8, 128), f32),
        dma((3, 2 * NX)), dma((3, 2 * NX)), dma((2, nz)), dma((2, nz)), dma((2, nz)), dma((2, nz)),
    ]
    scratch += [
        V((8, 128), f32), V((ntp, 8, 128), f32), dma((ntp,)), dma((ntp,)), V((rows, 256), f32),
        V((wide, 128), bf16), V((wide, 128), bf16), dma((nsp,)), dma((nsp,)),
    ]
    scratch += [V((3, 8, 128), f32), V((3, ntp, 8, 128), f32), dma((3, ntp)), dma((3, ntp))]
    scratch += [
        V((ny, 128, 256), bf16), V((ny, 128, 256), f32), V((ny, 128, 256), bf16),
        V((ny, 128, 128), bf16), V((ny, 128, 128), bf16), dma((ny,)), dma((ny,)), dma((ny,)), dma((ny,)),
    ]
    scratch += [V((wide, 128), bf16), V((wide, 128), bf16), dma((nsp,)), dma((nsp,))]
    hops = (2, half + 1, PIECES)
    scratch += [
        V((ny, rows, 256), bf16), dma(hops), dma(hops), dma(hops), dma(hops),
        V((rows, expert_gate.shape[2]), f32), V((rows, expert_gate.shape[2]), f32),
    ]
    scratch += [
        V((ny, rows, 128), bf16), V((ny, rows, 128), f32), V((ny, rows, 128), bf16), dma((ny,)), dma((ny,)),
        V((2, half, rows, 128), bf16), V((2, half, rows, 128), bf16), dma(hops), dma(hops),
    ]
    scratch += [V((wide, 128), bf16), V((wide, 128), bf16), dma((nsp,)), dma((nsp,))]
    return pl.pallas_call(
        functools.partial(layer_kernel, nsp, ntp),
        out_shape=jax.ShapeDtypeStruct((128, 128), bf16),
        in_specs=[hbm] * 20,
        out_specs=vmem,
        scratch_shapes=scratch,
        compiler_params=pltpu.CompilerParams(
            collective_id=0, has_side_effects=True, vmem_limit_bytes=62 * 1024 * 1024
        ),
        name="layer",
    )(*inputs, *weights)


def solution(mesh):
    in_specs = (
        P("sp", "tp"),
        P("sp", "tp"),
        P("sp", "tp", None),
        P("sp", "tp"),
        P("tp"),
        P("sp", "tp"),
        P("sp", "tp", None),
        P("sp", "tp"),
        P("tp"),
        P("tp", None),
        P("tp", None),
        P("tp"),
        P("tp"),
        P("sp", None),
        P("sp", None),
        P("sp", None, "tp"),
        P("sp", None, "tp"),
        P("sp", "tp", None),
        P("tp"),
        P("tp"),
    )
    step = functools.partial(body, mesh.shape["sp"], mesh.shape["tp"])
    return jax.shard_map(step, mesh=mesh, in_specs=in_specs, out_specs=P("sp", "tp"), check_vma=False)
```

```python
import functools
import jax
import jax.numpy as jnp
from jax import lax
from jax.experimental import pallas as pl
from jax.experimental.pallas import tpu as pltpu
from jax.sharding import PartitionSpec as P

depth_scale = 2.0**0.5
norm_eps = 1e-05
MESH = pl.DeviceIdType.MESH
NX = 4
CAP = 12
STRIDE = 16
PIECES = 4
PLANES = 2
bf16 = jnp.bfloat16
f32 = jnp.float32


def iota(shape, dim):
    return lax.broadcasted_iota(jnp.int32, shape, dim)


def ones_where(cond):
    return jnp.where(cond, 1.0, 0.0).astype(bf16)


def dot(a, b):
    return jnp.dot(a, b, preferred_element_type=f32)


def dot_tr(a, b):
    return lax.dot_general(a, b, (((1,), (1,)), ((), ())), preferred_element_type=f32)


def dot_tl(a, b):
    return lax.dot_general(a, b, (((0,), (0,)), ((), ())), preferred_element_type=f32)


def split(v, pieces):
    found = []
    for _ in range(pieces):
        part = v.astype(bf16)
        found.append(part)
        v = v - part.astype(f32)
    return found


def spread(rows8, low, high):
    parts = [p.astype(f32) for p in split(rows8, 3)] + [jnp.zeros_like(rows8)]
    stacked = jnp.concatenate(parts, axis=0).astype(bf16)
    row = iota((32, 256), 0)
    lane = iota((32, 256), 1)
    slot = row & 7
    pick = jnp.zeros((32, 256), jnp.bool_)
    for r, (first, last) in zip(low, high):
        pick = pick | ((slot == r) & (lane >= first) & (lane < last) & (row < 24))
    return dot_tl(stacked, ones_where(pick))


def rowsums(v):
    cat = jnp.concatenate(split(v, 3), axis=1)
    lane = iota((8, 768), 1) & 255
    row = iota((8, 768), 0)
    return dot_tr(ones_where((lane < 128) == (row < 4)), cat)


def rcopy(src, dst, send, recv, sp, tp):
    return pltpu.make_async_remote_copy(
        src_ref=src, dst_ref=dst, send_sem=send, recv_sem=recv, device_id=(sp, tp), device_id_type=MESH
    )


def loop(low, high, step):
    def run(i, carry):
        step(i)
        return carry

    lax.fori_loop(low, high, run, 0)


def near_order(n):
    return sorted(range(1, n), key=lambda d: (min(d, n - d), d))


def layer_kernel(
    nsp, ntp,
    qa_ref, qb_ref, ka_ref, kb_ref, oa_ref, ob_ref, res_ref, ga_ref, gb_ref, gs_ref, bs_ref, gf_ref, bf_ref,
    ids_ref, route_ref, pa_hbm, pb_hbm, wg_hbm, wu_hbm, wd_hbm, out_ref,
    held, hsem, pa, pb, wg, wu, wd, wsem, misc,
    kva, kvr, kvb, ofs, off, qba, qbb, ret, back, tot, tback,
    ks, kr, qs, qr, rs, rr, own_acc, own_gone,
    vec, vecs, vs_, vr_, mr, ssp, srv, ds2, dr2,
    stat, stats, ss, sr,
    p1s, p1o, p1v, p1r, p1i, p1ss, p1sr, p1rs, p1rr,
    dsp, drv, ds_, dr_,
    xg, as_, ar_, hs_, hr_, acc_g, acc_u,
    p2s, p2o, p2v, p2ss, p2sr, rb_s, rb_r, rbs_, rbr_,
    rts, rtv, ts_, tr_,
):
    sp, tp = lax.axis_index("sp"), lax.axis_index("tp")
    nz, ny = nsp // NX, ntp // 2
    z, x = lax.div(sp, NX), lax.rem(sp, NX)
    y, c = lax.div(tp, 2), lax.rem(tp, 2)
    mate = y * 2 + 1 - c
    columns = ntp * 128
    ends = []

    loads = [
        pltpu.make_async_copy(src, dst, wsem.at[i])
        for i, (src, dst) in enumerate(
            ((pa_hbm, pa), (pb_hbm, pb), (wg_hbm, wg), (wu_hbm, wu), (wd_hbm, wd))
        )
    ]
    given = (
        qa_ref, qb_ref, ka_ref, kb_ref, oa_ref, ob_ref, res_ref,
        ga_ref, gb_ref, gs_ref, bs_ref, gf_ref, bf_ref, ids_ref, route_ref,
    )
    fetches = [pltpu.make_async_copy(src, dst, hsem.at[i]) for i, (src, dst) in enumerate(zip(given, held))]
    for load in fetches:
        load.start()
    (
        qa_ref, qb_ref, ka_ref, kb_ref, oa_ref, ob_ref, res_ref,
        ga_ref, gb_ref, gs_ref, bs_ref, gf_ref, bf_ref, ids_ref, route_ref,
    ) = held

    barrier = pltpu.get_barrier_semaphore()

    def greet_sp(d):
        pl.semaphore_signal(barrier, 1, device_id=(lax.rem(sp + d, nsp), tp), device_id_type=MESH)

    def greet_tp(d):
        pl.semaphore_signal(barrier, 1, device_id=(sp, lax.rem(tp + d, ntp)), device_id_type=MESH)

    loop(1, nsp, greet_sp)
    loop(1, ntp, greet_tp)
    for load in fetches:
        load.wait()
    for load in loads:
        load.start()
    ofs[...] = jnp.zeros((8, 128), f32)
    ofs[0:2, :] = oa_ref[...]
    ofs[2:3, :] = ob_ref[...]
    vec[...] = jnp.zeros((8, 128), f32)
    vec[0:1, :] = gs_ref[...]
    vec[1:2, :] = bs_ref[...]
    pl.semaphore_wait(barrier, nsp - 1 + ntp - 1)

    groups = nz // PLANES
    zp, zb = lax.div(z, PLANES), lax.rem(z, PLANES)
    other_z = z + 1 - 2 * zb
    here_slot, there_slot = zb * NX, (1 - zb) * NX

    def key_copies(passed, k, slot, peer):
        rows = pl.ds(pl.multiple_of(slot * 128, 128), 128)
        sources = (kva.at[rows, :], kvb.at[rows, :], off.at[:, rows]) if passed else (ka_ref, kb_ref, ofs)
        targets = (kva.at[rows, :], kvb.at[rows, :], off.at[:, rows])
        return [
            rcopy(src, dst, ks.at[i, k], kr.at[i, k], peer, tp)
            for i, (src, dst) in enumerate(zip(sources, targets))
        ]

    def x_peer(d):
        return z * NX + lax.rem(x + d, NX)

    def cross_copies(slot):
        return key_copies(False, 0, slot + x, other_z * NX + x)

    def query_copies(dst_z, src_z):
        peer = dst_z * NX + x
        return (
            rcopy(qa_ref, qba.at[src_z], qs.at[0, dst_z], qr.at[0, src_z], peer, tp),
            rcopy(qb_ref, qbb.at[src_z], qs.at[1, dst_z], qr.at[1, src_z], peer, tp),
        )

    def result_copies(dst_z, src_z):
        peer = dst_z * NX + x
        return (
            rcopy(ret.at[dst_z], back.at[src_z], rs.at[0, dst_z], rr.at[0, src_z], peer, tp),
            rcopy(tot.at[dst_z], tback.at[src_z], rs.at[1, dst_z], rr.at[1, src_z], peer, tp),
        )

    for copy in cross_copies(here_slot):
        copy.start()

    def send_keys(d):
        for copy in key_copies(False, d, here_slot + x, x_peer(d)):
            copy.start()

    loop(1, NX, send_keys)

    def send_query(k):
        for copy in query_copies(z - PLANES * (k + 1), z):
            copy.start()

    loop(0, zp, send_query)

    def vec_copy(d):
        return rcopy(vec, vecs.at[tp], vs_.at[d], vr_.at[d], sp, lax.rem(tp + d, ntp))

    def vec_await(d):
        source = lax.rem(tp - d + ntp, ntp)
        rcopy(vec, vecs.at[source], vs_.at[d], vr_.at[d], sp, source).wait_recv()

    loop(1, ntp, lambda d: vec_copy(d).start())
    ends.append(lambda: loop(1, ntp, lambda d: vec_copy(d).wait_send()))
    vecs[tp] = vec[...]

    mine = pl.ds(pl.multiple_of((here_slot + x) * 128, 128), 128)
    kva[mine, :] = ka_ref[...]
    kvb[mine, :] = kb_ref[...]
    off[:, mine] = ofs[...]
    qba[z] = qa_ref[...]
    qbb[z] = qb_ref[...]

    for copy in cross_copies(there_slot):
        copy.wait_recv()

    def pass_keys(d):
        for copy in key_copies(True, NX + d, there_slot + x, x_peer(d)):
            copy.start()

    loop(1, NX, pass_keys)

    def await_keys(d):
        for copy in key_copies(False, d, here_slot + lax.rem(x - d + NX, NX), x_peer(d)):
            copy.wait_recv()

    def await_passed(d):
        for copy in key_copies(True, NX + d, there_slot + lax.rem(x - d + NX, NX), x_peer(d)):
            copy.wait_recv()

    def plane_rows(slot, b, blocks):
        return pl.ds(pl.multiple_of((slot + b) * 128, 128), blocks * 128)

    def swap_sides(slot):
        rows = plane_rows(slot, 0, NX)
        kvr[rows, :] = pltpu.roll(kva[rows, :].astype(f32), 64, 1).astype(bf16)

    lane = iota((128, 128), 1)
    gap = lane - iota((128, 128), 0)
    r256, c256 = iota((256, 256), 0) & 127, iota((256, 256), 1)
    later_matrix = ones_where((r256 > c256) | (c256 >= 128))
    first_lane = ones_where((iota((8, 384), 1) & 127) == 0)
    row8 = iota((8, 128), 0)

    def attend_blocks(zq, slot, blocks, masked, gones):
        qa, qb = (qba[zq].astype(f32) * 64.0**-0.5).astype(bf16), qbb[zq]
        zero = jnp.zeros_like(qa)
        accs, ends_ = [], []
        for h in range(3):
            q = (jnp.where(lane < 64, qa, zero), jnp.where(lane >= 64, qa, zero), qb)[h]
            gone = gones[h]
            weights = [None] * blocks
            for b in reversed(range(blocks)):
                rows = plane_rows(slot, b, 1)
                keys = (kva, kvr, kvb)[h][rows, :128]
                scores = dot_tr(q, keys)
                scores = (scores * 128.0**-0.5 if h == 2 else scores) + off[h : h + 1, rows]
                valid = gap < (x - b) * 128
                soft = jnp.maximum(scores, 0.0) + jnp.log(1.0 + jnp.exp(-jnp.abs(scores)))
                cat = jnp.concatenate(split(jnp.where(valid, soft, 0.0) if masked else soft, 2), axis=1)
                sums = dot(cat, later_matrix)
                power = (scores - soft) - (sums[:, :128] + gone)
                gone = gone + sums[:, 128:]
                weight = jnp.exp(power)
                weights[b] = (jnp.where(valid, weight, 0.0) if masked else weight).astype(bf16)
            rows = plane_rows(slot, 0, blocks)
            values = (kvr[rows, :], kva[rows, :], kvb[rows, 128:])[h]
            accs.append(dot(jnp.concatenate(weights, axis=1), values))
            ends_.append(gone)
        return jnp.concatenate([jnp.where(lane < 64, accs[0], accs[1]), accs[2]], axis=1), ends_

    def totals_of(gones):
        rows3 = [dot_tr(first_lane, jnp.concatenate(split(g, 3), axis=1)) for g in gones]
        return jnp.where(row8 == 0, rows3[0], jnp.where(row8 == 1, rows3[1], rows3[2]))

    nothing = [jnp.zeros((128, 128), f32)] * 3
    loop(1, NX, await_keys)
    swap_sides(here_slot)
    acc, gones = attend_blocks(z, here_slot, NX, True, nothing)
    own_acc[...] = acc
    for h in range(3):
        own_gone[h] = gones[h]
    loop(1, NX, await_passed)
    swap_sides(there_slot)

    @pl.when(zb == 1)
    def _():
        acc, gones = attend_blocks(z, 0, NX, False, [own_gone[h] for h in range(3)])
        own_acc[...] += acc
        for h in range(3):
            own_gone[h] = gones[h]

    back[z] = own_acc[...].astype(bf16)
    tback[z] = totals_of([own_gone[h] for h in range(3)])

    def visit(m):
        zq = z + PLANES * m
        for copy in query_copies(z, zq):
            copy.wait_recv()
        acc, gones = attend_blocks(zq, 0, PLANES * NX, False, nothing)
        ret[zq] = acc.astype(bf16)
        tot[zq] = totals_of(gones)
        for copy in result_copies(zq, z):
            copy.start()

    loop(1, groups - zp, visit)

    def gather(k, carry):
        acc, gone = carry
        zk = z - PLANES * k

        @pl.when(k > 0)
        def _():
            for copy in result_copies(z, zk):
                copy.wait_recv()

        wide = spread(jnp.exp(-gone), (0, 1, 2), ((0, 64), (64, 128), (128, 256)))
        return acc + wide * back[zk].astype(f32), gone + tback[zk]

    attend, _ = lax.fori_loop(
        0, zp + 1, gather, (jnp.zeros((128, 256), f32), jnp.zeros((8, 128), f32))
    )

    def end_attend():
        for copy in cross_copies(here_slot):
            copy.wait_send()

        def end_keys(d):
            for copy in key_copies(False, d, here_slot + x, x_peer(d)):
                copy.wait_send()
            for copy in key_copies(True, NX + d, there_slot + x, x_peer(d)):
                copy.wait_send()

        def end_query(k):
            for copy in query_copies(z - PLANES * (k + 1), z):
                copy.wait_send()

        def end_result(m):
            for copy in result_copies(z + PLANES * m, z):
                copy.wait_send()

        loop(1, NX, end_keys)
        loop(0, zp, end_query)
        loop(1, groups - zp, end_result)

    ends.append(end_attend)

    def stat_copy(n, d):
        return rcopy(stat.at[n], stats.at[n, d], ss.at[n, d], sr.at[n, d], sp, lax.rem(tp + d, ntp))

    def begin_tp(n, rows8):
        stat[n] = rows8
        loop(1, ntp, lambda d: stat_copy(n, d).start())
        ends.append(lambda: loop(1, ntp, lambda d: stat_copy(n, d).wait_send()))

    def finish_tp(n, rows8):
        loop(1, ntp, lambda d: stat_copy(n, d).wait_recv())
        total = rows8
        for d in range(1, ntp):
            total = total + stats[n, d]
        return total

    def halves_of(both):
        left, right = both[:, :128], both[:, 128:]
        return jnp.where(c == 0, left, right), jnp.where(c == 0, right, left)

    halves = ((0, 128), (128, 256))
    misc[...] = jnp.zeros((8, 128), f32)
    misc[0:2, :] = ids_ref[...].astype(f32)
    misc[2:4, :] = route_ref[...]
    facts = misc[...]
    id_cols = spread(facts, (0, 1), halves)
    route_cols = spread(facts, (2, 3), halves)
    lane128 = iota((128, 128), 1)
    lane_f = lane128.astype(f32)
    id_col = (id_cols[:, :128], id_cols[:, 128:])
    hot = [v == lane_f for v in id_col]
    tri = ones_where(iota((128, 128), 0) > lane128)
    earlier = dot(tri, ones_where(hot[0] | hot[1]))
    lane_all = iota((128, nsp * STRIDE), 1).astype(f32)
    choice = []
    for k in range(2):
        slot = jnp.sum(jnp.where(hot[k], earlier, 0.0), axis=1, keepdims=True)
        place = id_col[k][:, :1] * float(STRIDE) + slot
        choice.append(ones_where(place == lane_all))
    row_c, col_c = iota((nsp * CAP, nsp * STRIDE), 0), iota((nsp * CAP, nsp * STRIDE), 1)
    block_c = (row_c * (-(-(1 << 17) // CAP))) >> 17
    compact = ones_where(col_c == row_c + block_c * (STRIDE - CAP))

    own_squares = rowsums(attend * attend)
    begin_tp(0, own_squares)
    gained_a = (attend[:, :128] * ga_ref[...]).astype(bf16)
    gained_b = (attend[:, 128:] * gb_ref[...]).astype(bf16)
    loads[0].wait()
    loads[1].wait()

    def project(yy):
        cols = pl.ds(pl.multiple_of(yy * 256, 256), 256)
        return halves_of(dot(gained_a, pa[:, cols])), halves_of(dot(gained_b, pb[:, cols]))

    def mate1(d):
        return rcopy(p1s.at[d], p1v.at[d], p1ss.at[d], p1sr.at[d], sp, mate)

    def chip1(d):
        return rcopy(p1r.at[d], p1i.at[d], p1rs.at[d], p1rr.at[d], sp, lax.rem(y + d, ny) * 2 + c)

    def make1(d):
        (own_a, other_a), (own_b, other_b) = project(lax.rem(y + d, ny))
        p1s[d] = jnp.concatenate([other_a, other_b], axis=1).astype(bf16)
        mate1(d).start()
        p1o[d] = jnp.concatenate([own_a, own_b], axis=1)

    order = near_order(ny)[::-1]
    for d in order + [0]:
        make1(d)
    squares = finish_tp(0, own_squares)
    scale = spread(lax.rsqrt(squares / float(columns) + norm_eps), (0, 4), halves)

    def chip_sum(d):
        mate1(d).wait_recv()
        both = (p1o[d] + p1v[d].astype(f32)) * scale
        return both[:, :128] + both[:, 128:]

    for d in order:
        p1r[d] = chip_sum(d).astype(bf16)
        chip1(d).start()
    mixed = chip_sum(0)
    for d in order[::-1]:
        chip1(d).wait_recv()
        mixed = mixed + p1i[d].astype(f32)
    ends.append(lambda: loop(0, ny, lambda d: mate1(d).wait_send()))
    ends.append(lambda: loop(1, ny, lambda d: chip1(d).wait_send()))
    first = depth_scale * res_ref[...].astype(f32) + mixed.astype(bf16).astype(f32)

    def begin_norm(n, total):
        sums = rowsums(jnp.concatenate([total, total * total], axis=1))
        begin_tp(n, sums)
        return sums

    def moments(n, sums):
        sums = finish_tp(n, sums)
        mean = sums[0:1, :] / float(columns)
        var = sums[4:5, :] / float(columns) - mean * mean
        return spread(jnp.where(row8 < 4, mean, lax.rsqrt(var + norm_eps)), (0, 4), halves)

    def normed(total, wide, gain, bias):
        return ((total - wide[:, :128]) * wide[:, 128:] * gain + bias).astype(bf16)

    own_sums = begin_norm(1, first)

    here = pl.ds(pl.multiple_of(sp * STRIDE, STRIDE), STRIDE)

    def sp_copy(src, dst, send, recv, d):
        peer = lax.rem(sp + d, nsp)
        rows = pl.ds(pl.multiple_of(peer * STRIDE, STRIDE), STRIDE)
        return rcopy(src.at[rows, :], dst.at[here, :], send.at[d], recv.at[d], peer, tp)

    def sp_await(src, dst, send, recv, d):
        peer = lax.rem(sp - d + nsp, nsp)
        rows = pl.ds(pl.multiple_of(peer * STRIDE, STRIDE), STRIDE)
        rcopy(src.at[rows, :], dst.at[rows, :], send.at[d], recv.at[d], peer, tp).wait_recv()

    def post(src, dst, send, recv, value):
        src[...] = value
        loop(1, nsp, lambda d: sp_copy(src, dst, send, recv, d).start())
        ends.append(lambda: loop(1, nsp, lambda d: sp_copy(src, dst, send, recv, d).wait_send()))
        dst[here, :] = src[here, :]

    def collect(src, dst, send, recv):
        loop(1, nsp, lambda d: sp_await(src, dst, send, recv, d))
        return dst[...]

    routes = choice[0] + choice[1]
    post(dsp, drv, ds_, dr_, dot_tl(routes, first.astype(bf16)).astype(bf16))
    wide = moments(1, own_sums)
    pieces = split(wide[:, :128], 3) + split(wide[:, 128:], 3)
    packed = jnp.zeros((128, 128), f32)
    for i, piece in enumerate(pieces):
        packed = jnp.where(lane128 == i, piece.astype(f32), packed)
    post(ssp, srv, ds2, dr2, dot_tl(routes, packed.astype(bf16)).astype(bf16))
    settled = normed(first, wide, gs_ref[...], bs_ref[...])
    tokens = dot(compact, collect(dsp, drv, ds_, dr_)).astype(bf16)

    half = ny // 2
    height = nsp * CAP // PIECES
    ways = (0, 1)

    def chip_at(steps):
        return lax.rem(y + steps + ny, ny)

    def last_hop(way, p):
        return half if (p < PIECES // 2) == (way == 0) else half - 1

    def block_of(way, hop, core):
        source = chip_at(-hop if way == 0 else hop)
        return source, pl.ds(pl.multiple_of(core * 128, 128), 128)

    def along(way, hop, p):
        source, side = block_of(way, hop, c)
        block = xg.at[source, pl.ds(p * height, height), side]
        target = chip_at(1 if way == 0 else -1) * 2 + c
        return rcopy(block, block, as_.at[way, hop, p], ar_.at[way, hop + 1, p], sp, target)

    def along_await(way, hop, p):
        source, side = block_of(way, hop, c)
        block = xg.at[source, pl.ds(p * height, height), side]
        target = chip_at(-1 if way == 0 else 1) * 2 + c
        rcopy(block, block, as_.at[way, hop, p], ar_.at[way, hop, p], sp, target).wait_recv()

    def across(way, hop, p):
        source, side = block_of(way, hop, c)
        block = xg.at[source, pl.ds(p * height, height), side]
        return rcopy(block, block, hs_.at[way, hop, p], hr_.at[way, hop, p], sp, mate)

    def across_await(way, hop, p):
        source, side = block_of(way, hop, 1 - c)
        block = xg.at[source, pl.ds(p * height, height), side]
        rcopy(block, block, hs_.at[way, hop, p], hr_.at[way, hop, p], sp, mate).wait_recv()

    def take(source, start):
        rows = pl.ds(pl.multiple_of(source * 256, 256), 256)
        block = xg[source].astype(f32)
        mean, factor = mr[:, :128], mr[:, 128:]
        sides = []
        for i in range(2):
            gain, bias = vecs[source * 2 + i, 0:1, :], vecs[source * 2 + i, 1:2, :]
            sides.append((block[:, i * 128 : i * 128 + 128] - mean) * factor * gain + bias)
        block = jnp.concatenate(sides, axis=1).astype(bf16)
        gate, up = dot(block, wg[rows, :]), dot(block, wu[rows, :])
        if start:
            acc_g[...] = gate
            acc_u[...] = up
        else:
            acc_g[...] += gate
            acc_u[...] += up

    xg[y, :, pl.ds(pl.multiple_of(c * 128, 128), 128)] = tokens
    sends = [(way, 0, p) for p in range(PIECES) for way in ways if last_hop(way, p) > 0]
    crossings = [(0, 0, p) for p in range(PIECES)]
    for key in sends:
        along(*key).start()
    for key in crossings:
        across(*key).start()
    def advance(hop):
        reached = [(way, hop, p) for p in range(PIECES) for way in ways if hop <= last_hop(way, p)]
        for key in reached:
            way, _, p = key
            along_await(*key)
            if hop < last_hop(way, p):
                along(*key).start()
                sends.append(key)
            across(*key).start()
            crossings.append(key)
        return reached

    def consume(hop, reached):
        for key in reached:
            across_await(*key)
        take(chip_at(-hop), hop == 0)
        if 0 < hop < half:
            take(chip_at(hop), False)

    before = list(crossings)
    following = advance(1)
    loads[2].wait()
    loads[3].wait()
    loop(1, ntp, vec_await)
    row_m, col_m = iota((128, 256), 0), iota((128, 256), 1)
    unpack = ones_where(((row_m < 3) & (col_m < 128)) | ((row_m >= 3) & (row_m < 6) & (col_m >= 128)))
    numbers = dot(compact, collect(ssp, srv, ds2, dr2)).astype(bf16)
    mr[...] = dot(numbers, unpack)
    consume(0, before)
    for hop in range(1, half + 1):
        before = following
        if hop < half:
            following = advance(hop + 1)
        consume(hop, before)

    def end_gather():
        for key in sends:
            along(*key).wait_send()
        for key in crossings:
            across(*key).wait_send()

    ends.append(end_gather)

    gate = acc_g[...]
    hidden = (gate / (1.0 + jnp.exp(-gate)) * acc_u[...]).astype(bf16)
    loads[4].wait()

    def mate2(d):
        return rcopy(p2s.at[d], p2v.at[d], p2ss.at[d], p2sr.at[d], sp, mate)

    def make2(d):
        cols = pl.ds(pl.multiple_of(lax.rem(y + d, ny) * 256, 256), 256)
        own, other = halves_of(dot(hidden, wd[:, cols]))
        p2s[d] = other.astype(bf16)
        mate2(d).start()
        p2o[d] = own

    def term2(d, p):
        rows = slice(p * height, p * height + height)
        return p2o[d, rows, :] + p2v[d, rows, :].astype(f32)

    def pass2(way, step, p):
        rows = pl.ds(p * height, height)
        target = chip_at(1 if way == 0 else -1) * 2 + c
        return rcopy(
            rb_s.at[way, step, rows, :], rb_r.at[way, step, rows, :],
            rbs_.at[way, step, p], rbr_.at[way, step, p], sp, target,
        )

    passes = []

    def hand_on(step):
        left = half - step
        for p in range(PIECES):
            for way in ways:
                start = half - last_hop(way, p)
                if step < start:
                    continue
                rows = slice(p * height, p * height + height)
                value = term2(left if way == 0 else ny - left, p)
                if step > start:
                    pass2(way, step - 1, p).wait_recv()
                    value = value + rb_r[way, step - 1, rows, :].astype(f32)
                rb_s[way, step, rows, :] = value.astype(bf16)
                pass2(way, step, p).start()
                passes.append((way, step, p))

    make2(half)
    for step in range(half):
        left = half - step
        if left > 1:
            make2(left - 1)
            make2(ny - left + 1)
        else:
            make2(0)
        mate2(left).wait_recv()
        if left < half:
            mate2(ny - left).wait_recv()
        hand_on(step)
    mate2(0).wait_recv()
    outputs = []
    for p in range(PIECES):
        rows = slice(p * height, p * height + height)
        value = term2(0, p)
        for way in ways:
            if last_hop(way, p) > 0:
                pass2(way, half - 1, p).wait_recv()
                value = value + rb_r[way, half - 1, rows, :].astype(f32)
        outputs.append(value.astype(bf16))

    def end_sum():
        loop(0, ny, lambda d: mate2(d).wait_send())
        for key in passes:
            pass2(*key).wait_send()

    ends.append(end_sum)
    outputs = jnp.concatenate(outputs, axis=0)

    post(rts, rtv, ts_, tr_, dot_tl(compact, outputs).astype(bf16))
    returned = collect(rts, rtv, ts_, tr_)
    routed = route_cols[:, :128] * dot(choice[0], returned) + route_cols[:, 128:] * dot(choice[1], returned)
    second = depth_scale * settled.astype(f32) + routed
    last_sums = begin_norm(2, second)
    for end in ends[:-1]:
        end()
    out_ref[...] = normed(second, moments(2, last_sums), gf_ref[...], bf_ref[...])
    ends[-1]()


def body(
    nsp, ntp,
    residual_in, query_alpha, pairs_alpha, offset_alpha, gain_alpha,
    query_beta, pairs_beta, offset_beta, gain_beta, project_alpha, project_beta,
    gain_settle, bias_settle, expert_ids, route_weight,
    expert_gate, expert_up, expert_down, gain_final, bias_final,
):
    nz, ny = nsp // NX, ntp // 2
    vmem = pl.BlockSpec(memory_space=pltpu.VMEM)
    hbm = pl.BlockSpec(memory_space=pl.ANY)
    dma = pltpu.SemaphoreType.DMA
    V = pltpu.VMEM
    rows = nsp * CAP
    wide = nsp * STRIDE
    keys = PLANES * NX * 128
    half = ny // 2
    weights = (project_alpha, project_beta, expert_gate[0], expert_up[0], expert_down[0])
    vectors = [
        v.reshape(1, 128) for v in (gain_alpha, gain_beta, gain_settle, bias_settle, gain_final, bias_final)
    ]
    inputs = (
        query_alpha, query_beta, pairs_alpha.reshape(128, 128), pairs_beta.reshape(128, 256),
        offset_alpha.T, offset_beta.T, residual_in, *vectors, expert_ids.T, route_weight.T,
    )
    scratch = [tuple(V(a.shape, a.dtype) for a in inputs), dma((len(inputs),))]
    scratch += [V(w.shape, bf16) for w in weights] + [dma((5,)), V((8, 128), f32)]
    scratch += [
        V((keys, 128), bf16), V((keys, 128), bf16), V((keys, 256), bf16),
        V((8, 128), f32), V((8, keys), f32), V((nz, 128, 128), bf16), V((nz, 128, 128), bf16),
        V((nz, 128, 256), bf16), V((nz, 128, 256), bf16), V((nz, 8, 128), f32), V((nz, 8, 128), f32),
        dma((3, 2 * NX)), dma((3, 2 * NX)), dma((2, nz)), dma((2, nz)), dma((2, nz)), dma((2, nz)),
        V((128, 256), f32), V((3, 128, 128), f32),
    ]
    scratch += [
        V((8, 128), f32), V((ntp, 8, 128), f32), dma((ntp,)), dma((ntp,)), V((rows, 256), f32),
        V((wide, 128), bf16), V((wide, 128), bf16), dma((nsp,)), dma((nsp,)),
    ]
    scratch += [V((3, 8, 128), f32), V((3, ntp, 8, 128), f32), dma((3, ntp)), dma((3, ntp))]
    scratch += [
        V((ny, 128, 256), bf16), V((ny, 128, 256), f32), V((ny, 128, 256), bf16),
        V((ny, 128, 128), bf16), V((ny, 128, 128), bf16), dma((ny,)), dma((ny,)), dma((ny,)), dma((ny,)),
    ]
    scratch += [V((wide, 128), bf16), V((wide, 128), bf16), dma((nsp,)), dma((nsp,))]
    hops = (2, half + 1, PIECES)
    scratch += [
        V((ny, rows, 256), bf16), dma(hops), dma(hops), dma(hops), dma(hops),
        V((rows, expert_gate.shape[2]), f32), V((rows, expert_gate.shape[2]), f32),
    ]
    scratch += [
        V((ny, rows, 128), bf16), V((ny, rows, 128), f32), V((ny, rows, 128), bf16), dma((ny,)), dma((ny,)),
        V((2, half, rows, 128), bf16), V((2, half, rows, 128), bf16), dma(hops), dma(hops),
    ]
    scratch += [V((wide, 128), bf16), V((wide, 128), bf16), dma((nsp,)), dma((nsp,))]
    return pl.pallas_call(
        functools.partial(layer_kernel, nsp, ntp),
        out_shape=jax.ShapeDtypeStruct((128, 128), bf16),
        in_specs=[hbm] * 20,
        out_specs=vmem,
        scratch_shapes=scratch,
        compiler_params=pltpu.CompilerParams(
            collective_id=0, has_side_effects=True, vmem_limit_bytes=62 * 1024 * 1024
        ),
        name="layer",
    )(*inputs, *weights)


def solution(mesh):
    in_specs = (
        P("sp", "tp"),
        P("sp", "tp"),
        P("sp", "tp", None),
        P("sp", "tp"),
        P("tp"),
        P("sp", "tp"),
        P("sp", "tp", None),
        P("sp", "tp"),
        P("tp"),
        P("tp", None),
        P("tp", None),
        P("tp"),
        P("tp"),
        P("sp", None),
        P("sp", None),
        P("sp", None, "tp"),
        P("sp", None, "tp"),
        P("sp", "tp", None),
        P("tp"),
        P("tp"),
    )
    step = functools.partial(body, mesh.shape["sp"], mesh.shape["tp"])
    return jax.shard_map(step, mesh=mesh, in_specs=in_specs, out_specs=P("sp", "tp"), check_vma=False)
```
